32 devices in a mesh: fs: 8 (over z, x), tp: 4 (over y, core).
Axes of the slice: x: 2, y: 2, z: 4, core: 2. Of those that a mesh axis runs over, the one named last changes fastest.
Arguments:
- tokens: bfloat16 [6144, 2048], P('fs', 'tp'), may hold values from -6 to 6
- mix_gain: float32 [2048], replicated, may hold values from 0.1 to 1.9
- outer_gate: bfloat16 [2048, 2048], P('fs', 'tp'), may hold values from -0.125 to 0.125
- inner_gate: bfloat16 [2048, 2048], P('fs', 'tp'), may hold values from -0.125 to 0.125
- signal_in: bfloat16 [2048, 2048], P('fs', 'tp'), may hold values from -0.125 to 0.125
- mix_taps: float32 [3, 2048], P(None, 'tp'), may hold values from -3 to 3
- mix_bias: float32 [2048], P('tp'), may hold values from -3 to 3
- mix_out: bfloat16 [2048, 2048], P('tp', 'fs'), may hold values from -0.1875 to 0.1875
- ffn_gain: float32 [2048], replicated, may hold values from 0.1 to 1.9
- up_gate: bfloat16 [2048, 5632], P('fs', 'tp'), may hold values from -0.125 to 0.125
- up_value: bfloat16 [2048, 5632], P('fs', 'tp'), may hold values from -0.125 to 0.125
- ffn_taps: float32 [2, 3, 5632], P(None, None, 'tp'), may hold values from -3 to 3
- ffn_bias: float32 [2, 5632], P(None, 'tp'), may hold values from -3 to 3
- down_proj: bfloat16 [5632, 2048], P('tp', 'fs'), may hold values from -0.109375 to 0.109375
Outputs:
- layer_out: bfloat16 [6144, 2048], P('fs', 'tp')
The draws below stay inside these ranges and needn't reach their ends.
All inputs are finite; a program needn't handle non-finite values.
Results may differ from the reference program's by a relative error of at most 0.023.
Values may be sent and summed in bfloat16 or wider, within the bound.
A program may use at most 64 MiB of HBM per device.

```python
import jax
import jax.numpy as jnp
from jax import lax

D = 2048
W = 2048
FF = 5632
SEQLEN = 768
TOKENS = 6144
N_FS = 8
N_TP = 4


def with_spikes(array, key, source, target, shards_of, factor):
    owner, partner = [(jnp.arange(array.shape[position]) // (array.shape[position] // shards_of)).reshape([-1 if axis == position else 1 for axis in range(array.ndim)]) for position in (source, target)]
    chosen = jax.random.permutation(key, shards_of)[partner]
    strong = (owner == chosen) | (owner == (partner + shards_of // 2) % shards_of)
    return jnp.where(strong, factor * array, array)


def block_levels(own_key, dims, cuts, low, high):
    level, own = 1.0, jax.random.fold_in(own_key, 6)
    for dim, shards_of in cuts:
        heights = jnp.exp(jax.random.uniform(jax.random.fold_in(own, dim), (shards_of,), jnp.float32, low / len(cuts), high / len(cuts)))
        level = level * jnp.repeat(heights, dims[dim] // shards_of).reshape([-1 if axis == dim else 1 for axis in range(len(dims))])
    return level


def normal_values(own_key, shape, scale, bound, cuts=(), held_as=jnp.bfloat16):
    entries = scale * jax.random.normal(own_key, shape, jnp.float32)
    if cuts:
        entries = entries * block_levels(own_key, shape, cuts, -0.22, 0.18)
    return jnp.clip(entries, -bound, bound).astype(held_as)


def heavy_noise(rng, shape, deviation, bound, cuts, heavy, held_as=jnp.bfloat16):
    values = deviation * jax.random.normal(rng, shape, jnp.float32)
    if cuts:
        values = values * block_levels(rng, shape, cuts, -0.22, 0.18)
    return jnp.clip(with_spikes(values, jax.random.fold_in(rng, 3), *heavy), -bound, bound).astype(held_as)


def setup_inputs(seed: int = 0) -> dict:
    key_of = jax.random.split(jax.random.key(seed), 15)
    tokens = normal_values(key_of[0], (TOKENS, D), 1.0, 6.0, ((0, 8), (1, 4)))
    mix_gain = jnp.clip(1.0 + 0.18 * jax.random.normal(key_of[1], (D,), jnp.float32), 0.1, 1.9)
    outer_gate = normal_values(key_of[2], (D, W), D ** -0.5, 0.125, ((0, 8), (1, 4)))
    inner_gate = normal_values(key_of[3], (D, W), D ** -0.5, 0.125, ((0, 8), (1, 4)))
    signal_in = normal_values(key_of[4], (D, W), D ** -0.5, 0.125, ((0, 8), (1, 4)))
    mix_taps = normal_values(key_of[5], (3, W), 0.577, 3.0, ((1, 4),), jnp.float32)
    mix_bias = normal_values(key_of[6], (W,), 0.5, 3.0, ((0, 4),), jnp.float32)
    mix_out = heavy_noise(key_of[7], (W, D), W ** -0.5, 0.1875, ((0, 4), (1, 8)), (0, 1, 8, 2.0))
    ffn_gain = jnp.clip(1.0 + 0.18 * jax.random.normal(key_of[8], (D,), jnp.float32), 0.1, 1.9)
    up_gate = normal_values(key_of[9], (D, FF), D ** -0.5, 0.125, ((0, 8), (1, 4)))
    up_value = normal_values(key_of[10], (D, FF), D ** -0.5, 0.125, ((0, 8), (1, 4)))
    ffn_taps = normal_values(key_of[11], (2, 3, FF), 0.577, 3.0, ((2, 4),), jnp.float32)
    ffn_bias = normal_values(key_of[12], (2, FF), 0.5, 3.0, ((1, 4),), jnp.float32)
    down_proj = heavy_noise(key_of[13], (FF, D), FF ** -0.5, 0.109375, ((0, 4), (1, 8)), (0, 1, 8, 2.0))
    return {"tokens": tokens, "mix_gain": mix_gain, "outer_gate": outer_gate, "inner_gate": inner_gate, "signal_in": signal_in, "mix_taps": mix_taps, "mix_bias": mix_bias, "mix_out": mix_out, "ffn_gain": ffn_gain, "up_gate": up_gate, "up_value": up_value, "ffn_taps": ffn_taps, "ffn_bias": ffn_bias, "down_proj": down_proj}


EPS = 1e-06

def rms_rows(values, gain):
    floats = values.astype(jnp.float32)
    scaled = floats * lax.rsqrt(lax.optimization_barrier(jnp.mean(floats * floats, axis=-1, keepdims=True)) + EPS) * gain
    return scaled.astype(jnp.bfloat16)

def causal_taps(signal, taps, bias):
    shaped = signal.reshape(N_FS, SEQLEN, signal.shape[-1])
    first = jnp.pad(shaped, ((0, 0), (1, 0), (0, 0)))[:, :-1]
    second = jnp.pad(shaped, ((0, 0), (2, 0), (0, 0)))[:, :-2]
    result = taps[2] * shaped + taps[1] * first + taps[0] * second + bias
    return result.reshape(signal.shape)

def group_sum(active, weight):
    width = active.shape[1] // N_TP
    total = jnp.zeros((active.shape[0], weight.shape[1]), jnp.float32)
    for group in range(N_TP):
        term = jnp.dot(active[:, group * width:(group + 1) * width], weight[group * width:(group + 1) * width], preferred_element_type=jnp.float32)
        total = total + lax.optimization_barrier(term.astype(jnp.bfloat16)).astype(jnp.float32)
    return total

def reference(tokens, mix_gain, outer_gate, inner_gate, signal_in, mix_taps, mix_bias, mix_out, ffn_gain, up_gate, up_value, ffn_taps, ffn_bias, down_proj):
    normed = rms_rows(tokens, mix_gain)
    outer = jnp.dot(normed, outer_gate, preferred_element_type=jnp.float32).astype(jnp.bfloat16)
    inner = jnp.dot(normed, inner_gate, preferred_element_type=jnp.float32).astype(jnp.bfloat16)
    signal = jnp.dot(normed, signal_in, preferred_element_type=jnp.float32).astype(jnp.bfloat16)
    mixed_in = inner.astype(jnp.float32) * signal.astype(jnp.float32)
    gated = (outer.astype(jnp.float32) * causal_taps(mixed_in, mix_taps, mix_bias)).astype(jnp.bfloat16)
    mixed = group_sum(gated, mix_out)
    hidden_state = (tokens.astype(jnp.float32) + mixed).astype(jnp.bfloat16)
    normed_two = rms_rows(hidden_state, ffn_gain)
    gate_pre = jnp.dot(normed_two, up_gate, preferred_element_type=jnp.float32).astype(jnp.bfloat16)
    value_pre = jnp.dot(normed_two, up_value, preferred_element_type=jnp.float32).astype(jnp.bfloat16)
    gate_conv = causal_taps(gate_pre.astype(jnp.float32), ffn_taps[0], ffn_bias[0])
    value_conv = causal_taps(value_pre.astype(jnp.float32), ffn_taps[1], ffn_bias[1])
    active = (jax.nn.silu(gate_conv) * value_conv).astype(jnp.bfloat16)
    fed = group_sum(active, down_proj)
    return (hidden_state.astype(jnp.float32) + fed).astype(jnp.bfloat16)
```

```python
import functools

import jax
import jax.numpy as jnp
from jax import lax
from jax.experimental import pallas as pl
from jax.experimental.pallas import tpu as pltpu
from jax.sharding import PartitionSpec as P

EPS = 1e-06
F32, BF16 = jnp.float32, jnp.bfloat16
MESH = pl.DeviceIdType.MESH
UP, DOWN, RIGHT, LEFT = range(4)


def grid_of(n_fs):
    nx = 1
    while nx * nx * 4 <= n_fs:
        nx *= 2
    return n_fs // nx, nx


def tiles(extent, width, body):
    whole = extent // width
    if whole:
        @pl.loop(0, whole)
        def _(i):
            body(i, pl.multiple_of(i * width, width), width)
    if extent % width:
        body(whole, whole * width, extent % width)


def causal(v, taps, bias):
    row = lax.broadcasted_iota(jnp.int32, v.shape, 0)
    first = jnp.where(row < 1, 0.0, pltpu.roll(v, 1, axis=0))
    second = jnp.where(row < 2, 0.0, pltpu.roll(v, 2, axis=0))
    return taps[2] * v + taps[1] * first + taps[0] * second + bias


def kernel(
    n_fs, n_tp, tok_in, og, ig, si, mo, ug, uv, dp,
    mix_gain, ffn_gain, mix_taps, mix_bias, ffn_taps, ffn_bias,
    out,
    w0, w1, w2, w3, f0, f1, f2,
    tok, normed, state, outer, inner, signal, gate, value,
    part1, sib1, rs1, part2, sib2, rs2,
    load_sem, send_sem, recv_sem, fsend, ffar, frecv,
    tok_sib, tok_y, tok_recv, st_sib, st_y, st_z, st_recv,
    s1_send, s1_recv, p1_send, p1_recv, s2_send, s2_recv, p2_send, p2_recv,
):
    nz, nx = grid_of(n_fs)
    fs, tp = lax.axis_index("fs"), lax.axis_index("tp")
    z, x = fs // nx, fs % nx
    ny = n_tp // 2
    y, core = tp // 2, tp % 2
    mate = tp + 1 - 2 * core
    pair = (z + 1 - 2 * (z % 2)) * nx + x
    bufs = (w0, w1, w2, w3)
    fbufs = (f0, f1, f2)
    fowns = (ug, uv, dp)
    rows, own = tok.shape[2], tok.shape[3]
    per = n_fs // n_tp
    wide = part1.shape[3]
    hidden = ug.shape[1]
    big = f0.shape[2]
    small = hidden - big
    outside = jnp.logical_or(z == 0, z == nz - 1)
    inside = jnp.logical_not(outside)

    ways = (
        (z < nz - 1, fs + nx),
        (z > 0, fs - nx),
        (x < nx - 1, fs + 1),
        (x > 0, fs - 1),
    )
    barrier = pltpu.get_barrier_semaphore()
    expected = n_tp - 1 + nz - 1 + ny - 1
    for there, peer in ways[2:]:
        expected = expected + jnp.where(there, 1, 0)

        @pl.when(there)
        def _(peer=peer):
            pl.semaphore_signal(barrier, inc=1, device_id={"fs": peer}, device_id_type=MESH)
    for r in range(1, nz):
        pl.semaphore_signal(barrier, inc=1, device_id={"fs": (z + r) % nz * nx + x}, device_id_type=MESH)
    for r in range(1, n_tp):
        pl.semaphore_signal(barrier, inc=1, device_id={"tp": (tp + r) % n_tp}, device_id_type=MESH)
    ypeers = [(y + r) % ny for r in range(1, ny)]
    for yy in ypeers:
        pl.semaphore_signal(
            barrier, inc=1, device_id={"fs": pair, "tp": yy * 2 + core}, device_id_type=MESH
        )

    loads = [pltpu.make_async_copy(a, b.at[fs], load_sem.at[i]) for i, (a, b) in enumerate(zip((og, ig, si, mo), bufs))]
    loads.append(pltpu.make_async_copy(tok_in, tok.at[0, tp], load_sem.at[4]))
    for c in loads:
        c.start()

    def span(p):
        return (0, big) if p else (big, small)

    def held(w, p, block):
        size = span(p)[1]
        return fbufs[w].at[block, pl.ds(0, size)] if w == 2 else fbufs[w].at[block, :, pl.ds(0, size)]

    def source(w, p):
        start, size = span(p)
        return fowns[w].at[pl.ds(start, size)] if w == 2 else fowns[w].at[:, pl.ds(start, size)]

    def each_part(body):
        @pl.when(outside)
        def _():
            body(0)

        @pl.when(inside)
        def _():
            body(1)

    def own_f(w, starting):
        def body(p):
            c = pltpu.make_async_copy(source(w, p), held(w, p, fs), load_sem.at[5 + w])
            if starting:
                c.start()
            else:
                c.wait()
        each_part(body)

    for w in range(3):
        own_f(w, True)
    if small < big:
        @pl.when(outside)
        def _():
            for w in range(2):
                fbufs[w][:, :, small:big] = jnp.zeros((n_fs, f0.shape[1], big - small), BF16)
            f2[:, small:big, :] = jnp.zeros((n_fs, big - small, wide), BF16)
    pl.semaphore_wait(barrier, expected)

    def cut(w):
        r = bufs[w].shape[1]
        a = max(16, (r * 13 // 16) // 16 * 16)
        return ((0, a), (a, r - a))

    def piece(w, k, block, way):
        start, size = cut(w)[k]
        ref = bufs[w].at[block, pl.ds(start, size)]
        return pltpu.make_async_remote_copy(
            src_ref=ref, dst_ref=ref,
            send_sem=send_sem.at[w, k, block, way], recv_sem=recv_sem.at[w, k, block],
            device_id={"fs": ways[way][1]}, device_id_type=MESH,
        )

    def arrive(w, k, block):
        piece(w, k, block, UP).wait_recv()

    def run(cond, c, sending):
        @pl.when(cond)
        def _():
            if sending:
                c.start()
            else:
                c.wait_send()

    def go(w, k, block, way, cond, sending):
        run(jnp.logical_and(cond, ways[way][0]), piece(w, k, block, way), sending)

    yes = z >= 0
    steps = 2 * nz - 1

    def layer(i):
        half = (i + 1) // 2
        z0 = z + jnp.where(i % 2 == 1, -half, half)
        return z0, jnp.logical_and(z0 >= 0, z0 < nz)

    def along_z(w, i, sending):
        z0, valid = layer(i)
        away = z0 != z

        @pl.when(valid)
        def _():
            mine = z0 * nx + x

            def both(k, block):
                go(w, k, block, UP, z0 <= z, sending)
                go(w, k, block, DOWN, z0 >= z, sending)

            if sending:
                @pl.when(away)
                def _():
                    arrive(w, 0, mine)
            both(0, mine)
            go(w, 0, mine, RIGHT, yes, sending)
            go(w, 0, mine, LEFT, yes, sending)
            level = jnp.logical_not(away)

            @pl.loop(0, nx)
            def _(j):
                x0 = (x + j) % nx
                if sending:
                    @pl.when(jnp.logical_or(away, x != x0))
                    def _():
                        arrive(w, 1, z0 * nx + x0)
                go(w, 1, z0 * nx + x0, RIGHT, jnp.logical_and(level, x0 <= x), sending)
                go(w, 1, z0 * nx + x0, LEFT, jnp.logical_and(level, x0 >= x), sending)
                both(1, z0 * nx + x0)

    def sides(body):
        for dist in range(1, nx):
            for sign in (-1, 1):
                x0 = x + sign * dist

                @pl.when(jnp.logical_and(x0 >= 0, x0 < nx))
                def _(sign=sign, x0=x0):
                    body(x0, RIGHT if sign < 0 else LEFT)

    def along_x(w, i, sending):
        z0, valid = layer(i)

        @pl.when(valid)
        def _():
            def body(x0, way):
                if sending:
                    arrive(w, 0, z0 * nx + x0)
                go(w, 0, z0 * nx + x0, way, yes, sending)
            sides(body)

    def step(w, i):
        @pl.when(i == 1)
        def _():
            row(w)

        @pl.when(i < steps)
        def _():
            along_z(w, i, True)
        along_x(w, i - 1, True)

    def pump(w, lo=1, hi=steps + 1):
        @pl.loop(lo, hi)
        def _(i):
            step(w, i)

    def spaced(move, lo, hi):
        def hook(j, total):
            first, last = j * (hi - lo) // total, (j + 1) * (hi - lo) // total

            @pl.loop(first, last)
            def _(i):
                move(lo + i)
        return hook

    def during(w, lo, hi):
        return spaced(lambda i: step(w, i), lo, hi)

    def begin(w):
        loads[w].wait()
        for k in (1, 0):
            for way in (RIGHT, LEFT, UP, DOWN):
                go(w, k, fs, way, yes, True)

    def row(w):
        def body(x0, way):
            block = z * nx + x0
            arrive(w, 1, block)
            for to in (way, UP, DOWN):
                go(w, 1, block, to, yes, True)
        sides(body)

    def fcopy(w, p, block, src, target, sem):
        return pltpu.make_async_remote_copy(
            src_ref=src, dst_ref=held(w, p, block), send_sem=sem, recv_sem=frecv.at[w, block],
            device_id={"fs": target}, device_id_type=MESH,
        )

    def fgo(w, p, block, src, way, cond, sending):
        there, target = ways[way]
        run(jnp.logical_and(cond, there), fcopy(w, p, block, src, target, fsend.at[w, block, way]), sending)

    def farrive(w, p, block):
        fcopy(w, p, block, held(w, p, block), fs, fsend.at[w, block, 0]).wait_recv()

    up_in = jnp.logical_and(z + 1 >= 1, z + 1 <= nz - 2)
    down_in = jnp.logical_and(z - 1 >= 1, z - 1 <= nz - 2)

    def begin_fx(w, sending=True):
        for p, cond in ((0, outside), (1, inside)):
            for way in (RIGHT, LEFT):
                fgo(w, p, fs, source(w, p), way, cond, sending)

    def begin_fz(w, sending=True):
        fgo(w, 1, fs, source(w, 1), UP, up_in, sending)
        fgo(w, 1, fs, source(w, 1), DOWN, down_in, sending)
        for e, end in enumerate((0, nz - 1)):
            run(z != end, fcopy(w, 0, fs, source(w, 0), end * nx + x, ffar.at[w, e]), sending)

    def frelay(w, i, sending=True):
        z0, valid = layer(i)
        block = z0 * nx + x

        @pl.when(jnp.logical_and(valid, z0 != z))
        def _():
            def body(p):
                ref = held(w, p, block)
                if sending:
                    farrive(w, p, block)
                if p:
                    fgo(w, p, block, ref, UP, jnp.logical_and(z0 < z, up_in), sending)
                    fgo(w, p, block, ref, DOWN, jnp.logical_and(z0 > z, down_in), sending)
                fgo(w, p, block, ref, RIGHT, yes, sending)
                fgo(w, p, block, ref, LEFT, yes, sending)
            each_part(body)

    def fside(w, i, sending=True):
        z0, valid = layer(i)

        @pl.when(valid)
        def _():
            def part(p):
                def body(x0, way):
                    block = z0 * nx + x0
                    if sending:
                        farrive(w, p, block)
                    fgo(w, p, block, held(w, p, block), way, yes, sending)
                sides(body)
            each_part(part)

    def frelays(w, lo, hi):
        @pl.loop(lo, hi)
        def _(i):
            frelay(w, i)

    def fduring(w, lo, hi):
        return spaced(lambda i: frelay(w, i), lo, hi)

    def fsides(w):
        @pl.loop(0, steps)
        def _(i):
            fside(w, i)

    def send(ref, send, recv, to):
        return pltpu.make_async_remote_copy(
            src_ref=ref[0], dst_ref=ref[1], send_sem=send, recv_sem=recv, device_id=to, device_id_type=MESH
        )

    def got(ref, recv):
        send((ref, ref), st_z.at[0], recv, {"tp": mate}).wait_recv()

    def to_mate(buf, s, t, sib, recv):
        return send((buf.at[s, t], buf.at[s, t]), sib.at[s, t], recv.at[s, t], {"tp": mate})

    def to_ys(buf, s, ysend, recv):
        ref = buf.at[s, tp]
        return [
            send((ref, ref), ysend.at[s, r], recv.at[s, tp], {"tp": yy * 2 + core})
            for r, yy in enumerate(ypeers)
        ]

    def ag_out(buf, s, sib, ysend, recv):
        for c in to_ys(buf, s, ysend, recv):
            c.start()
        to_mate(buf, s, tp, sib, recv).start()

    def ag_relay(buf, s, sib, recv):
        for yy in ypeers:
            t = yy * 2 + core
            got(buf.at[s, t], recv.at[s, t])
            to_mate(buf, s, t, sib, recv).start()

    def ag_done(buf, s, recv):
        for yy in range(ny):
            t = yy * 2 + 1 - core
            got(buf.at[s, t], recv.at[s, t])

    def ag_sent(buf, s, sib, ysend, recv):
        for c in to_ys(buf, s, ysend, recv):
            c.wait_send()
        for yy in range(ny):
            to_mate(buf, s, yy * 2 + core, sib, recv).wait_send()

    def norm(buf, s, gain, hook):
        high = 64

        @pl.loop(0, rows // high)
        def _(m):
            at = pl.ds(pl.multiple_of(m * high, high), high)
            total = jnp.zeros((high, 1), F32)
            for t in range(n_tp):
                v = buf[s, t, at, :].astype(F32)
                total = total + jnp.sum(v * v, axis=-1, keepdims=True)
            scale = lax.rsqrt(total / (n_tp * own) + EPS)
            for t in range(n_tp):
                cols = slice(t * own, (t + 1) * own)
                v = buf[s, t, at, :].astype(F32)
                normed[s, at, cols] = (v * scale * gain[:, cols]).astype(BF16)
            hook(m, rows // high)

    mt = 256 if rows % 256 == 0 else rows

    def none(j, total):
        pass

    def project(weights, s, dst, hook):
        n, r, c = weights.shape
        mts = rows // mt
        pieces = -(-c // 256) * mts

        def column(index, start, size):
            @pl.loop(0, mts)
            def _(m):
                at = pl.ds(pl.multiple_of(m * mt, mt), mt)
                weight = weights[:, :, pl.ds(start, size)].reshape(n * r, size)
                dst[s, at, pl.ds(start, size)] = jnp.dot(
                    normed[s, at, :], weight, preferred_element_type=F32
                ).astype(BF16)
                hook(index * mts + m, pieces)
        tiles(c, 256, column)

    def owner(block):
        t = block // per
        return t // 2, t % 2, block % per

    def out_block(weights, act, seqs, part, sib, ssend, srecv, block):
        for s in range(seqs):
            @pl.loop(0, rows // mt)
            def _(m):
                at = pl.ds(pl.multiple_of(m * mt, mt), mt)
                part[block, s, at, :] = jnp.dot(
                    act[s, at, :], weights[block], preferred_element_type=F32
                ).astype(BF16)
        yo, co, k = owner(block)
        run(co != core, mate_copy(part, sib, ssend, srecv, block), True)

    def mate_copy(part, sib, ssend, srecv, block):
        yo, co, k = owner(block)
        slot = yo * per + k
        return send((part.at[block], sib.at[slot]), ssend.at[slot], srecv.at[slot], {"tp": mate})

    def home_copy(part, s, rs, psend, precv, block, rel):
        yo, co, k = owner(block)
        to = {"tp": yo * 2 + core} if rel == 0 else {"fs": pair, "tp": yo * 2 + core}
        return send((part.at[block, s], rs.at[rel, y, k]), psend.at[rel, yo, k], precv.at[rel, y, k], to)

    def combine(seqs, part, sib, rs, srecv, psend, precv, block):
        yo, co, k = owner(block)
        slot = yo * per + k

        @pl.when(co == core)
        def _():
            got(sib.at[slot], srecv.at[slot])
            high = 128
            for s in reversed(range(seqs)):
                @pl.loop(0, rows // high)
                def _(m):
                    at = pl.ds(pl.multiple_of(m * high, high), high)
                    part[block, s, at, :] = (
                        part[block, s, at, :].astype(F32) + sib[slot, s, at, :].astype(F32)
                    ).astype(BF16)
                run(yes if s else yo != y, home_copy(part, s, rs, psend, precv, block, s), True)

    def sent_home(seqs, part, sib, rs, ssend, srecv, psend, precv):
        @pl.loop(0, n_fs)
        def _(block):
            yo, co, k = owner(block)
            run(co != core, mate_copy(part, sib, ssend, srecv, block), False)
            for s in range(seqs):
                run(
                    co == core if s else jnp.logical_and(co == core, yo != y),
                    home_copy(part, s, rs, psend, precv, block, s), False,
                )

    def add_up(base, seqs, part, rs, precv, dst):
        for rel in range(seqs):
            for yy in (ypeers if rel == 0 else ypeers + [y]):
                for k in range(per):
                    got(rs.at[rel, yy, k], precv.at[rel, yy, k])
        high = 128

        @pl.loop(0, rows // high)
        def _(m):
            at = pl.ds(pl.multiple_of(m * high, high), high)
            for k in range(per):
                cols = slice(k * wide, (k + 1) * wide)
                total = part[tp * per + k, 0, at, :].astype(F32)
                for rel in range(seqs):
                    for yy in (ypeers if rel == 0 else ypeers + [y]):
                        total = total + rs[rel, yy, k, at, :].astype(F32)
                dst[at, cols] = (base[at, cols].astype(F32) + total).astype(BF16)

    def sweep(move, form, merge):
        @pl.loop(0, steps + 2)
        def _(i):
            move(i)

            def blocks(i, body):
                @pl.loop(0, nx)
                def _(j):
                    i0 = jnp.where(j == 0, i, i - 1)
                    z0, good = layer(i0)
                    good = jnp.logical_and(good, jnp.logical_and(i0 >= 0, i0 < steps))

                    @pl.when(good)
                    def _():
                        body(z0 * nx + (x + j) % nx)
            blocks(i, form)
            blocks(i - 1, merge)

    tok_sems = (tok_sib, tok_y, tok_recv)
    st_sems = (st_sib, st_y, st_recv)

    begin(0)
    begin(1)
    loads[4].wait()
    ag_out(tok, 0, *tok_sems)
    pump(0)
    begin(2)
    ag_relay(tok, 0, tok_sib, tok_recv)
    pump(1, 1, 3)
    ag_done(tok, 0, tok_recv)
    norm(tok, 0, mix_gain, during(1, 3, 6))
    project(w0, 0, outer, during(1, 6, steps + 1))
    begin(3)
    project(w1, 0, inner, during(2, 1, 4))
    pump(2, 4)
    begin_fx(0)
    begin_fz(0)
    project(w2, 0, signal, during(3, 1, 3))

    def mixer(index, start, size):
        cols = pl.ds(start, size)
        taps = [mix_taps[j:j + 1, cols] for j in range(3)]
        v = inner[0, :, cols].astype(F32) * signal[0, :, cols].astype(F32)
        outer[0, :, cols] = (outer[0, :, cols].astype(F32) * causal(v, taps, mix_bias[:, cols])).astype(BF16)
    tiles(outer.shape[2], 128, mixer)

    def move1(i):
        @pl.when(jnp.logical_and(i >= 3, i <= steps))
        def _():
            step(3, i)
    sweep(
        move1,
        lambda b: out_block(w3, outer, 1, part1, sib1, s1_send, s1_recv, b),
        lambda b: combine(1, part1, sib1, rs1, s1_recv, p1_send, p1_recv, b),
    )
    begin_fx(1)
    frelays(0, 1, 3)
    add_up(tok.at[0, tp], 1, part1, rs1, p1_recv, state.at[0, tp])
    to_pair = send((state.at[0, tp], state.at[1, tp]), st_z.at[0], st_recv.at[1, tp], {"fs": pair})
    to_pair.start()
    ag_out(state, 0, *st_sems)
    begin_fz(1)
    frelays(0, 3, steps)
    ag_relay(state, 0, st_sib, st_recv)
    frelays(1, 1, 3)
    got(state.at[1, tp], st_recv.at[1, tp])
    ag_out(state, 1, *st_sems)
    begin_fx(2)
    begin_fz(2)
    ag_done(state, 0, st_recv)
    norm(state, 0, ffn_gain, none)
    for w in range(3):
        own_f(w, False)
    fsides(0)
    project(f0, 0, gate, fduring(1, 3, 5))
    ag_relay(state, 1, st_sib, st_recv)
    ag_done(state, 1, st_recv)
    norm(state, 1, ffn_gain, fduring(1, 5, steps))
    project(f0, 1, gate, fduring(2, 1, 3))
    fsides(1)
    project(f1, 0, value, none)
    project(f1, 1, value, none)
    shift = jnp.where(outside, big, 0)

    @pl.loop(0, jnp.where(outside, small, big) // 128)
    def _(i):
        cols = pl.ds(pl.multiple_of(i * 128, 128), 128)
        at = pl.ds(pl.multiple_of(shift + i * 128, 128), 128)
        for s in range(2):
            g = causal(gate[s, :, cols].astype(F32), [ffn_taps[j:j + 1, at] for j in range(3)], ffn_bias[0:1, at])
            v = causal(value[s, :, cols].astype(F32), [ffn_taps[j:j + 1, at] for j in range(3, 6)], ffn_bias[1:2, at])
            gate[s, :, cols] = (g / (1.0 + jnp.exp(-g)) * v).astype(BF16)

    def move2(i):
        @pl.when(jnp.logical_and(i >= 3, i < steps))
        def _():
            frelay(2, i)

        @pl.when(jnp.logical_and(i >= 1, i <= steps))
        def _():
            fside(2, i - 1)
    sweep(
        move2,
        lambda b: out_block(f2, gate, 2, part2, sib2, s2_send, s2_recv, b),
        lambda b: combine(2, part2, sib2, rs2, s2_recv, p2_send, p2_recv, b),
    )
    add_up(state.at[0, tp], 2, part2, rs2, p2_recv, out)

    to_pair.wait_send()
    ag_sent(tok, 0, *tok_sems)
    ag_sent(state, 0, *st_sems)
    ag_sent(state, 1, *st_sems)
    sent_home(1, part1, sib1, rs1, s1_send, s1_recv, p1_send, p1_recv)
    sent_home(2, part2, sib2, rs2, s2_send, s2_recv, p2_send, p2_recv)
    for w in range(4):
        @pl.loop(0, steps)
        def _(i):
            along_z(w, i, False)
            along_x(w, i, False)
    for w in range(3):
        begin_fx(w, False)
        begin_fz(w, False)

        @pl.loop(0, steps)
        def _(i):
            frelay(w, i, False)
            fside(w, i, False)


def solution(mesh):
    n_fs, n_tp = mesh.shape["fs"], mesh.shape["tp"]

    def on_device(
        tokens, mix_gain, outer_gate, inner_gate, signal_in, mix_taps, mix_bias, mix_out,
        ffn_gain, up_gate, up_value, ffn_taps, ffn_bias, down_proj,
    ):
        rows, own = tokens.shape
        ffn_taps = ffn_taps.reshape(6, -1)
        spare = -up_gate.shape[1] % 128
        if spare:
            up_gate, up_value, ffn_taps, ffn_bias = (
                jnp.pad(a, ((0, 0), (0, spare))) for a in (up_gate, up_value, ffn_taps, ffn_bias)
            )
            down_proj = jnp.pad(down_proj, ((0, spare), (0, 0)))
        weights = (outer_gate, inner_gate, signal_in, mix_out)
        chan, hidden = outer_gate.shape[1], up_gate.shape[1]
        depth, wide = outer_gate.shape[0], mix_out.shape[1]
        big = hidden - hidden // 256 * 128
        model = own * n_tp
        hbm = pl.BlockSpec(memory_space=pl.ANY)
        vmem = pl.BlockSpec(memory_space=pltpu.VMEM)
        dma = pltpu.SemaphoreType.DMA
        per, ny = n_fs // n_tp, n_tp // 2
        return pl.pallas_call(
            functools.partial(kernel, n_fs, n_tp),
            out_shape=jax.ShapeDtypeStruct(tokens.shape, BF16),
            in_specs=[hbm] * 8 + [vmem] * 6,
            out_specs=vmem,
            scratch_shapes=[pltpu.VMEM((n_fs, *w.shape), BF16) for w in weights]
            + [
                pltpu.VMEM((n_fs, depth, big), BF16),
                pltpu.VMEM((n_fs, depth, big), BF16),
                pltpu.VMEM((n_fs, big, wide), BF16),
                pltpu.VMEM((1, n_tp, rows, own), BF16),
                pltpu.VMEM((2, rows, model), BF16),
                pltpu.VMEM((2, n_tp, rows, own), BF16),
                pltpu.VMEM((1, rows, chan), BF16),
                pltpu.VMEM((1, rows, chan), BF16),
                pltpu.VMEM((1, rows, chan), BF16),
                pltpu.VMEM((2, rows, big), BF16),
                pltpu.VMEM((2, rows, big), BF16),
                pltpu.VMEM((n_fs, 1, rows, wide), BF16),
                pltpu.VMEM((ny * per, 1, rows, wide), BF16),
                pltpu.VMEM((1, ny, per, rows, wide), BF16),
                pltpu.VMEM((n_fs, 2, rows, wide), BF16),
                pltpu.VMEM((ny * per, 2, rows, wide), BF16),
                pltpu.VMEM((2, ny, per, rows, wide), BF16),
                dma((8,)),
                dma((4, 2, n_fs, 4)),
                dma((4, 2, n_fs)),
                dma((3, n_fs, 4)),
                dma((3, 2)),
                dma((3, n_fs)),
                dma((1, n_tp)), dma((1, ny)), dma((1, n_tp)),
                dma((2, n_tp)), dma((2, ny)), dma((1,)), dma((2, n_tp)),
                dma((ny * per,)), dma((ny * per,)), dma((1, ny, per)), dma((1, ny, per)),
                dma((ny * per,)), dma((ny * per,)), dma((2, ny, per)), dma((2, ny, per)),
            ],
            compiler_params=pltpu.CompilerParams(
                collective_id=0, has_side_effects=True, vmem_limit_bytes=67043328
            ),
        )(
            tokens, *weights, up_gate, up_value, down_proj, mix_gain[None], ffn_gain[None], mix_taps, mix_bias[None],
            ffn_taps, ffn_bias,
        )

    return jax.shard_map(
        on_device,
        mesh=mesh,
        in_specs=(
            P("fs", "tp"), P(), P("fs", "tp"), P("fs", "tp"), P("fs", "tp"), P(None, "tp"), P("tp"),
            P("tp", "fs"), P(), P("fs", "tp"), P("fs", "tp"), P(None, None, "tp"), P(None, "tp"),
            P("tp", "fs"),
        ),
        out_specs=P("fs", "tp"),
        check_vma=False,
    )
```

```python
import functools

import jax
import jax.numpy as jnp
from jax import lax
from jax.experimental import pallas as pl
from jax.experimental.pallas import tpu as pltpu
from jax.sharding import PartitionSpec as P

EPS = 1e-06
F32, BF16 = jnp.float32, jnp.bfloat16
MESH = pl.DeviceIdType.MESH
UP, DOWN, RIGHT, LEFT = range(4)


def grid_of(n_fs):
    nx = 1
    while nx * nx * 4 <= n_fs:
        nx *= 2
    return n_fs // nx, nx


def tiles(extent, width, body):
    whole = extent // width
    if whole:
        @pl.loop(0, whole)
        def _(i):
            body(i, pl.multiple_of(i * width, width), width)
    if extent % width:
        body(whole, whole * width, extent % width)


def causal(v, taps, bias):
    row = lax.broadcasted_iota(jnp.int32, v.shape, 0)
    first = jnp.where(row < 1, 0.0, pltpu.roll(v, 1, axis=0))
    second = jnp.where(row < 2, 0.0, pltpu.roll(v, 2, axis=0))
    return taps[2] * v + taps[1] * first + taps[0] * second + bias


def kernel(
    n_fs, n_tp, tok_in, og, ig, si, mo, ug, uv, dp,
    mix_gain, ffn_gain, mix_taps, mix_bias, ffn_taps, ffn_bias,
    out,
    w0, w1, w2, w3, f0, f1, f2,
    tok, normed, state, outer, inner, signal, gate, value,
    part1, sib1, rs1, part2, sib2, rs2, far2,
    load_sem, send_sem, recv_sem, fsend, ffar, frecv,
    tok_sib, tok_y, tok_recv, st_sib, st_y, st_z, st_recv,
    s1_send, s1_recv, p1_send, p1_recv, s2_send, s2_recv, p2_send, p2_recv, far_send, far_recv,
):
    nz, nx = grid_of(n_fs)
    fs, tp = lax.axis_index("fs"), lax.axis_index("tp")
    z, x = fs // nx, fs % nx
    ny = n_tp // 2
    y, core = tp // 2, tp % 2
    mate = tp + 1 - 2 * core
    pair = (z + 1 - 2 * (z % 2)) * nx + x
    bufs = (w0, w1, w2, w3)
    fbufs = (f0, f1, f2)
    fowns = (ug, uv, dp)
    rows, own = tok.shape[2], tok.shape[3]
    per = n_fs // n_tp
    wide = part1.shape[3]
    hidden = ug.shape[1]
    big = f0.shape[2]
    small = hidden - big
    outside = jnp.logical_or(z == 0, z == nz - 1)
    inside = jnp.logical_not(outside)

    ways = (
        (z < nz - 1, fs + nx),
        (z > 0, fs - nx),
        (x < nx - 1, fs + 1),
        (x > 0, fs - 1),
    )
    barrier = pltpu.get_barrier_semaphore()
    expected = n_tp - 1 + nz - 1 + ny - 1
    for there, peer in ways[2:]:
        expected = expected + jnp.where(there, 1, 0)

        @pl.when(there)
        def _(peer=peer):
            pl.semaphore_signal(barrier, inc=1, device_id={"fs": peer}, device_id_type=MESH)
    for r in range(1, nz):
        pl.semaphore_signal(barrier, inc=1, device_id={"fs": (z + r) % nz * nx + x}, device_id_type=MESH)
    for r in range(1, n_tp):
        pl.semaphore_signal(barrier, inc=1, device_id={"tp": (tp + r) % n_tp}, device_id_type=MESH)
    ypeers = [(y + r) % ny for r in range(1, ny)]
    for yy in ypeers:
        pl.semaphore_signal(
            barrier, inc=1, device_id={"fs": pair, "tp": yy * 2 + core}, device_id_type=MESH
        )

    loads = [pltpu.make_async_copy(a, b.at[fs], load_sem.at[i]) for i, (a, b) in enumerate(zip((og, ig, si, mo), bufs))]
    loads.append(pltpu.make_async_copy(tok_in, tok.at[0, tp], load_sem.at[4]))
    for c in loads:
        c.start()

    def span(p):
        return (0, big) if p else (big, small)

    def held(w, p, block):
        size = span(p)[1]
        return fbufs[w].at[block, pl.ds(0, size)] if w == 2 else fbufs[w].at[block, :, pl.ds(0, size)]

    def source(w, p):
        start, size = span(p)
        return fowns[w].at[pl.ds(start, size)] if w == 2 else fowns[w].at[:, pl.ds(start, size)]

    def each_part(body):
        @pl.when(outside)
        def _():
            body(0)

        @pl.when(inside)
        def _():
            body(1)

    def own_f(w, starting):
        def body(p):
            c = pltpu.make_async_copy(source(w, p), held(w, p, fs), load_sem.at[5 + w])
            if starting:
                c.start()
            else:
                c.wait()
        each_part(body)

    for w in range(3):
        own_f(w, True)
    if small < big:
        @pl.when(outside)
        def _():
            for w in range(2):
                fbufs[w][:, :, small:big] = jnp.zeros((n_fs, f0.shape[1], big - small), BF16)
            f2[:, small:big, :] = jnp.zeros((n_fs, big - small, wide), BF16)
    pl.semaphore_wait(barrier, expected)

    def cut(w):
        r = bufs[w].shape[1]
        a = max(16, (r * 13 // 16) // 16 * 16)
        return ((0, a), (a, r - a))

    def piece(w, k, block, way):
        start, size = cut(w)[k]
        ref = bufs[w].at[block, pl.ds(start, size)]
        return pltpu.make_async_remote_copy(
            src_ref=ref, dst_ref=ref,
            send_sem=send_sem.at[w, k, block, way], recv_sem=recv_sem.at[w, k, block],
            device_id={"fs": ways[way][1]}, device_id_type=MESH,
        )

    def arrive(w, k, block):
        piece(w, k, block, UP).wait_recv()

    def run(cond, c, sending):
        @pl.when(cond)
        def _():
            if sending:
                c.start()
            else:
                c.wait_send()

    def go(w, k, block, way, cond, sending):
        run(jnp.logical_and(cond, ways[way][0]), piece(w, k, block, way), sending)

    yes = z >= 0
    steps = nz
    near = jnp.minimum(z, nz - 1 - z)

    def layer(i):
        beside = z + jnp.where(i % 2 == 1, -((i + 1) // 2), i // 2)
        beyond = jnp.where(z < nz // 2, z + i - near, z - i + near)
        return jnp.where(i <= 2 * near, beside, beyond)

    def order(q):
        return ((y + 1) * (nz // ny) + q) % nz

    def spread_z(w, k, block, z0, sending):
        go(w, k, block, UP, z0 <= z, sending)
        go(w, k, block, DOWN, z0 >= z, sending)

    def along_z(w, k, i, sending):
        z0 = layer(i)

        @pl.when(i > 0)
        def _():
            def relay(block):
                if sending:
                    arrive(w, k, block)
                spread_z(w, k, block, z0, sending)
            if k == 0:
                relay(z0 * nx + x)
                go(w, 0, z0 * nx + x, RIGHT, yes, sending)
                go(w, 0, z0 * nx + x, LEFT, yes, sending)
            else:
                @pl.loop(0, nx)
                def _(j):
                    relay(z0 * nx + (x + j) % nx)

    def sides(body):
        for dist in range(1, nx):
            for sign in (-1, 1):
                x0 = x + sign * dist

                @pl.when(jnp.logical_and(x0 >= 0, x0 < nx))
                def _(sign=sign, x0=x0):
                    body(x0, RIGHT if sign < 0 else LEFT)

    def along_x(w, z0, sending):
        def body(x0, way):
            if sending:
                arrive(w, 0, z0 * nx + x0)
            go(w, 0, z0 * nx + x0, way, yes, sending)
        sides(body)

    def step(w, i):
        @pl.when(i == 0)
        def _():
            row(w)

        @pl.when(jnp.logical_and(i > 0, i < steps))
        def _():
            along_z(w, 0, i, True)

        @pl.when(i >= steps)
        def _():
            along_z(w, 1, i - steps + 1, True)

    total_steps = 2 * steps - 1

    def pump(w, lo=0, hi=total_steps):
        @pl.loop(lo, hi)
        def _(i):
            step(w, i)

    def across(w):
        @pl.loop(0, steps)
        def _(i):
            along_x(w, layer(i), True)

    def spaced(move, lo, hi):
        def hook(j, total):
            first, last = j * (hi - lo) // total, (j + 1) * (hi - lo) // total

            @pl.loop(first, last)
            def _(i):
                move(lo + i)
        return hook

    def during(w, lo, hi):
        return spaced(lambda i: step(w, i), lo, hi)

    def begin(w, sending=True):
        if sending:
            loads[w].wait()
        for k in (1, 0):
            go(w, k, fs, RIGHT, yes, sending)
            go(w, k, fs, LEFT, yes, sending)
            spread_z(w, k, fs, z, sending)

    def row(w, sending=True):
        def body(x0, way):
            block = z * nx + x0
            if sending:
                arrive(w, 1, block)
            go(w, 1, block, way, yes, sending)
            spread_z(w, 1, block, z, sending)
        sides(body)

    def fcopy(w, p, block, src, target, sem):
        return pltpu.make_async_remote_copy(
            src_ref=src, dst_ref=held(w, p, block), send_sem=sem, recv_sem=frecv.at[w, block],
            device_id={"fs": target}, device_id_type=MESH,
        )

    def fgo(w, p, block, src, way, cond, sending):
        there, target = ways[way]
        run(jnp.logical_and(cond, there), fcopy(w, p, block, src, target, fsend.at[w, block, way]), sending)

    def farrive(w, p, block):
        fcopy(w, p, block, held(w, p, block), fs, fsend.at[w, block, 0]).wait_recv()

    up_in = jnp.logical_and(z + 1 >= 1, z + 1 <= nz - 2)
    down_in = jnp.logical_and(z - 1 >= 1, z - 1 <= nz - 2)

    def begin_fx(w, sending=True):
        for p, cond in ((0, outside), (1, inside)):
            for way in (RIGHT, LEFT):
                fgo(w, p, fs, source(w, p), way, cond, sending)

    def begin_fb(w, sending=True):
        fgo(w, 1, fs, source(w, 1), UP, up_in, sending)
        fgo(w, 1, fs, source(w, 1), DOWN, down_in, sending)

    def begin_fa(w, lo, hi, sending=True):
        for e, end in enumerate((0, nz - 1)):
            apart = abs(z - end)
            run(
                jnp.logical_and(apart >= lo, apart <= hi),
                fcopy(w, 0, fs, source(w, 0), end * nx + x, ffar.at[w, e]), sending,
            )

    def frelay(w, i, p):
        @pl.when(inside if p else outside)
        def _():
            frelay_part(w, layer(i), p)

    def frelay_part(w, z0, p, sending=True):
        block = z0 * nx + x
        ref = held(w, p, block)

        @pl.when(z0 != z)
        def _():
            if sending:
                farrive(w, p, block)
            if p:
                fgo(w, p, block, ref, UP, jnp.logical_and(z0 < z, up_in), sending)
                fgo(w, p, block, ref, DOWN, jnp.logical_and(z0 > z, down_in), sending)
            fgo(w, p, block, ref, RIGHT, yes, sending)
            fgo(w, p, block, ref, LEFT, yes, sending)

    def fside(w, z0, sending=True):
        def part(p):
            def body(x0, way):
                block = z0 * nx + x0
                if sending:
                    farrive(w, p, block)
                fgo(w, p, block, held(w, p, block), way, yes, sending)
            sides(body)
        each_part(part)

    def fdo(*list_):
        def hook(j, total):
            for n, (w, i, p) in enumerate(list_):
                @pl.when(j == n * total // len(list_))
                def _(w=w, i=i, p=p):
                    frelay(w, i, p)
        return hook

    def fsides(w):
        @pl.loop(0, steps)
        def _(i):
            fside(w, layer(i))

    def send(ref, send, recv, to):
        return pltpu.make_async_remote_copy(
            src_ref=ref[0], dst_ref=ref[1], send_sem=send, recv_sem=recv, device_id=to, device_id_type=MESH
        )

    def got(ref, recv):
        send((ref, ref), st_z.at[0], recv, {"tp": mate}).wait_recv()

    def to_mate(buf, s, t, sib, recv):
        return send((buf.at[s, t], buf.at[s, t]), sib.at[s, t], recv.at[s, t], {"tp": mate})

    def to_ys(buf, s, ysend, recv):
        ref = buf.at[s, tp]
        return [
            send((ref, ref), ysend.at[s, r], recv.at[s, tp], {"tp": yy * 2 + core})
            for r, yy in enumerate(ypeers)
        ]

    def ag_out(buf, s, sib, ysend, recv):
        for c in to_ys(buf, s, ysend, recv):
            c.start()
        to_mate(buf, s, tp, sib, recv).start()

    def ag_relay(buf, s, sib, recv):
        for yy in ypeers:
            t = yy * 2 + core
            got(buf.at[s, t], recv.at[s, t])
            to_mate(buf, s, t, sib, recv).start()

    def ag_done(buf, s, recv):
        for yy in range(ny):
            t = yy * 2 + 1 - core
            got(buf.at[s, t], recv.at[s, t])

    def ag_sent(buf, s, sib, ysend, recv):
        for c in to_ys(buf, s, ysend, recv):
            c.wait_send()
        for yy in range(ny):
            to_mate(buf, s, yy * 2 + core, sib, recv).wait_send()

    def norm(buf, s, gain, hook):
        high = 64

        @pl.loop(0, rows // high)
        def _(m):
            at = pl.ds(pl.multiple_of(m * high, high), high)
            total = jnp.zeros((high, 1), F32)
            for t in range(n_tp):
                v = buf[s, t, at, :].astype(F32)
                total = total + jnp.sum(v * v, axis=-1, keepdims=True)
            scale = lax.rsqrt(total / (n_tp * own) + EPS)
            for t in range(n_tp):
                cols = slice(t * own, (t + 1) * own)
                v = buf[s, t, at, :].astype(F32)
                normed[s, at, cols] = (v * scale * gain[:, cols]).astype(BF16)
            hook(m, rows // high)

    mt = rows

    def none(j, total):
        pass

    def project(weights, s, dst, hook):
        n, r, c = weights.shape
        mts = rows // mt
        pieces = -(-c // 256) * mts

        def column(index, start, size):
            @pl.loop(0, mts)
            def _(m):
                at = pl.ds(pl.multiple_of(m * mt, mt), mt)
                weight = weights[:, :, pl.ds(start, size)].reshape(n * r, size)
                dst[s, at, pl.ds(start, size)] = jnp.dot(
                    normed[s, at, :], weight, preferred_element_type=F32
                ).astype(BF16)
                hook(index * mts + m, pieces)
        tiles(c, 256, column)

    def owner(block):
        t = block // per
        return t // 2, t % 2, block % per

    def out_block(weights, act, part, sib, ssend, srecv, s, block):
        @pl.loop(0, rows // mt)
        def _(m):
            at = pl.ds(pl.multiple_of(m * mt, mt), mt)
            part[block, s, at, :] = jnp.dot(
                act[s, at, :], weights[block], preferred_element_type=F32
            ).astype(BF16)
        yo, co, k = owner(block)
        run(co != core, mate_copy(part, sib, ssend, srecv, s, block), True)

    def mate_copy(part, sib, ssend, srecv, s, block):
        yo, co, k = owner(block)
        slot = yo * per + k
        return send((part.at[block, s], sib.at[slot, s]), ssend.at[slot, s], srecv.at[slot, s], {"tp": mate})

    def home_copy(part, rs, psend, precv, s, block):
        yo, co, k = owner(block)
        return send(
            (part.at[block, s], rs.at[y, k, s]), psend.at[yo, k, s], precv.at[y, k, s], {"tp": yo * 2 + core}
        )

    high = 128

    def row_tiles(body):
        @pl.loop(0, rows // high)
        def _(m):
            body(pl.ds(pl.multiple_of(m * high, high), high))

    def combine(part, sib, rs, srecv, psend, precv, s, block):
        yo, co, k = owner(block)
        slot = yo * per + k

        @pl.when(co == core)
        def _():
            got(sib.at[slot, s], srecv.at[slot, s])

            def add(at):
                part[block, s, at, :] = (
                    part[block, s, at, :].astype(F32) + sib[slot, s, at, :].astype(F32)
                ).astype(BF16)
            row_tiles(add)
            run(yo != y, home_copy(part, rs, psend, precv, s, block), True)

    def sent_home(seqs, part, sib, rs, ssend, srecv, psend, precv):
        @pl.loop(0, n_fs)
        def _(block):
            yo, co, k = owner(block)
            for s in range(seqs):
                run(co != core, mate_copy(part, sib, ssend, srecv, s, block), False)
                run(jnp.logical_and(co == core, yo != y), home_copy(part, rs, psend, precv, s, block), False)

    def collected(rs, precv):
        for k in range(per):
            for yy in ypeers:
                got(rs.at[yy, k, 0], precv.at[yy, k, 0])

    def share(part, rs, k, s, at):
        total = part[tp * per + k, s, at, :].astype(F32)
        for yy in ypeers:
            total = total + rs[yy, k, s, at, :].astype(F32)
        return total

    def add_up(base, part, rs, dst, far):
        def add(at):
            for k in range(per):
                cols = slice(k * wide, (k + 1) * wide)
                total = share(part, rs, k, 0, at)
                if far is not None:
                    total = total + far[k, at, :].astype(F32)
                dst[at, cols] = (base[at, cols].astype(F32) + total).astype(BF16)
        row_tiles(add)

    def cross_copy(k):
        return send((part2.at[tp * per + k, 1], far2.at[k]), far_send.at[k], far_recv.at[k], {"fs": pair})

    def cross():
        for k in range(per):
            for yy in ypeers:
                got(rs2.at[yy, k, 1], p2_recv.at[yy, k, 1])

            def add(at):
                part2[tp * per + k, 1, at, :] = share(part2, rs2, k, 1, at).astype(BF16)
            row_tiles(add)
            cross_copy(k).start()

    def crossed():
        for k in range(per):
            got(far2.at[k], far_recv.at[k])

    def sweep(move, form, merge):
        @pl.loop(0, nz + 2)
        def _(q):
            move(q)

            def blocks(q, body):
                @pl.loop(0, nx)
                def _(j):
                    at = jnp.where(j == 0, q, q - 1)

                    @pl.when(jnp.logical_and(at >= 0, at < nz))
                    def _():
                        body(order(at) * nx + (x + j) % nx)
            blocks(q, form)
            blocks(q - 1, merge)

    tok_sems = (tok_sib, tok_y, tok_recv)
    st_sems = (st_sib, st_y, st_recv)

    begin(0)
    begin(1)
    loads[4].wait()
    ag_out(tok, 0, *tok_sems)
    pump(0)
    begin(2)
    ag_relay(tok, 0, tok_sib, tok_recv)
    pump(1)
    begin(3)
    begin_fb(0)
    ag_done(tok, 0, tok_recv)
    norm(tok, 0, mix_gain, during(2, 0, 2))
    across(0)
    project(w0, 0, outer, during(2, 2, total_steps))
    across(1)
    project(w1, 0, inner, during(3, 0, steps))
    begin_fx(0)
    across(2)
    project(w2, 0, signal, during(3, steps, total_steps))
    begin_fa(0, 1, 1)
    frelay(0, 1, 1)
    frelay(0, 2, 1)

    def mixer(index, start, size):
        cols = pl.ds(start, size)
        taps = [mix_taps[j:j + 1, cols] for j in range(3)]
        v = inner[0, :, cols].astype(F32) * signal[0, :, cols].astype(F32)
        outer[0, :, cols] = (outer[0, :, cols].astype(F32) * causal(v, taps, mix_bias[:, cols])).astype(BF16)
    tiles(outer.shape[2], 128, mixer)

    def move1(q):
        @pl.when(jnp.logical_and(q >= 1, q <= nz))
        def _():
            along_x(3, order(q - 1), True)
    sweep(
        move1,
        lambda b: out_block(w3, outer, part1, sib1, s1_send, s1_recv, 0, b),
        lambda b: combine(part1, sib1, rs1, s1_recv, p1_send, p1_recv, 0, b),
    )
    begin_fb(1)
    begin_fa(0, 2, nz)
    begin_fx(1)
    frelay(0, 3, 1)
    collected(rs1, p1_recv)
    add_up(tok.at[0, tp], part1, rs1, state.at[0, tp], None)
    to_pair = send((state.at[0, tp], state.at[1, tp]), st_z.at[0], st_recv.at[1, tp], {"fs": pair})
    to_pair.start()
    ag_out(state, 0, *st_sems)
    begin_fb(2)
    frelay(1, 1, 1)
    frelay(1, 2, 1)
    frelay(0, 1, 0)
    frelay(0, 2, 0)
    frelay(0, 3, 0)
    ag_relay(state, 0, st_sib, st_recv)
    begin_fa(1, 1, 1)
    frelay(1, 3, 1)
    got(state.at[1, tp], st_recv.at[1, tp])
    ag_out(state, 1, *st_sems)
    ag_done(state, 0, st_recv)
    norm(state, 0, ffn_gain, none)
    for w in range(3):
        own_f(w, False)
    fsides(0)
    project(f0, 0, gate, none)
    begin_fa(1, 2, 2)
    frelay(1, 1, 0)
    begin_fa(1, 3, nz)
    frelay(1, 2, 0)
    ag_relay(state, 1, st_sib, st_recv)
    ag_done(state, 1, st_recv)
    frelay(1, 3, 0)
    begin_fx(2)
    begin_fa(2, 1, 1)
    norm(state, 1, ffn_gain, none)
    frelay(2, 1, 1)
    frelay(2, 2, 1)
    project(f0, 1, gate, none)
    begin_fa(2, 2, 2)
    frelay(2, 3, 1)
    fsides(1)
    begin_fa(2, 3, nz)
    project(f1, 0, value, none)
    frelay(2, 1, 0)
    project(f1, 1, value, none)
    frelay(2, 2, 0)
    shift = jnp.where(outside, big, 0)

    @pl.loop(0, jnp.where(outside, small, big) // 128)
    def _(i):
        cols = pl.ds(pl.multiple_of(i * 128, 128), 128)
        at = pl.ds(pl.multiple_of(shift + i * 128, 128), 128)
        for s in range(2):
            g = causal(gate[s, :, cols].astype(F32), [ffn_taps[j:j + 1, at] for j in range(3)], ffn_bias[0:1, at])
            v = causal(value[s, :, cols].astype(F32), [ffn_taps[j:j + 1, at] for j in range(3, 6)], ffn_bias[1:2, at])
            gate[s, :, cols] = (g / (1.0 + jnp.exp(-g)) * v).astype(BF16)

    frelay(2, 3, 0)

    def move2(q):
        @pl.when(jnp.logical_and(q >= 1, q <= nz))
        def _():
            fside(2, order(q - 1))

    def sweep2(s):
        sweep(
            move2 if s else (lambda q: None),
            lambda b: out_block(f2, gate, part2, sib2, s2_send, s2_recv, s, b),
            lambda b: combine(part2, sib2, rs2, s2_recv, p2_send, p2_recv, s, b),
        )
    sweep2(1)
    sweep2(0)
    cross()
    crossed()
    collected(rs2, p2_recv)
    add_up(state.at[0, tp], part2, rs2, out, far2)

    to_pair.wait_send()
    ag_sent(tok, 0, *tok_sems)
    ag_sent(state, 0, *st_sems)
    ag_sent(state, 1, *st_sems)
    for k in range(per):
        cross_copy(k).wait_send()
    sent_home(1, part1, sib1, rs1, s1_send, s1_recv, p1_send, p1_recv)
    sent_home(2, part2, sib2, rs2, s2_send, s2_recv, p2_send, p2_recv)
    for w in range(4):
        begin(w, False)
        row(w, False)

        @pl.loop(0, steps)
        def _(i):
            along_z(w, 0, i, False)
            along_z(w, 1, i, False)
            along_x(w, i, False)
    for w in range(3):
        begin_fx(w, False)
        begin_fb(w, False)
        begin_fa(w, 1, nz, False)

        @pl.loop(0, steps)
        def _(i):
            each_part(lambda p: frelay_part(w, i, p, False))
            fside(w, i, False)


def solution(mesh):
    n_fs, n_tp = mesh.shape["fs"], mesh.shape["tp"]

    def on_device(
        tokens, mix_gain, outer_gate, inner_gate, signal_in, mix_taps, mix_bias, mix_out,
        ffn_gain, up_gate, up_value, ffn_taps, ffn_bias, down_proj,
    ):
        rows, own = tokens.shape
        ffn_taps = ffn_taps.reshape(6, -1)
        spare = -up_gate.shape[1] % 128
        if spare:
            up_gate, up_value, ffn_taps, ffn_bias = (
                jnp.pad(a, ((0, 0), (0, spare))) for a in (up_gate, up_value, ffn_taps, ffn_bias)
            )
            down_proj = jnp.pad(down_proj, ((0, spare), (0, 0)))
        weights = (outer_gate, inner_gate, signal_in, mix_out)
        chan, hidden = outer_gate.shape[1], up_gate.shape[1]
        depth, wide = outer_gate.shape[0], mix_out.shape[1]
        big = hidden - hidden // 256 * 128
        model = own * n_tp
        hbm = pl.BlockSpec(memory_space=pl.ANY)
        vmem = pl.BlockSpec(memory_space=pltpu.VMEM)
        dma = pltpu.SemaphoreType.DMA
        per, ny = n_fs // n_tp, n_tp // 2
        return pl.pallas_call(
            functools.partial(kernel, n_fs, n_tp),
            out_shape=jax.ShapeDtypeStruct(tokens.shape, BF16),
            in_specs=[hbm] * 8 + [vmem] * 6,
            out_specs=vmem,
            scratch_shapes=[pltpu.VMEM((n_fs, *w.shape), BF16) for w in weights]
            + [
                pltpu.VMEM((n_fs, depth, big), BF16),
                pltpu.VMEM((n_fs, depth, big), BF16),
                pltpu.VMEM((n_fs, big, wide), BF16),
                pltpu.VMEM((1, n_tp, rows, own), BF16),
                pltpu.VMEM((2, rows, model), BF16),
                pltpu.VMEM((2, n_tp, rows, own), BF16),
                pltpu.VMEM((1, rows, chan), BF16),
                pltpu.VMEM((1, rows, chan), BF16),
                pltpu.VMEM((1, rows, chan), BF16),
                pltpu.VMEM((2, rows, big), BF16),
                pltpu.VMEM((2, rows, big), BF16),
                pltpu.VMEM((n_fs, 1, rows, wide), BF16),
                pltpu.VMEM((ny * per, 1, rows, wide), BF16),
                pltpu.VMEM((ny, per, 1, rows, wide), BF16),
                pltpu.VMEM((n_fs, 2, rows, wide), BF16),
                pltpu.VMEM((ny * per, 2, rows, wide), BF16),
                pltpu.VMEM((ny, per, 2, rows, wide), BF16),
                pltpu.VMEM((per, rows, wide), BF16),
                dma((8,)),
                dma((4, 2, n_fs, 4)),
                dma((4, 2, n_fs)),
                dma((3, n_fs, 4)),
                dma((3, 2)),
                dma((3, n_fs)),
                dma((1, n_tp)), dma((1, ny)), dma((1, n_tp)),
                dma((2, n_tp)), dma((2, ny)), dma((1,)), dma((2, n_tp)),
                dma((ny * per, 1)), dma((ny * per, 1)), dma((ny, per, 1)), dma((ny, per, 1)),
                dma((ny * per, 2)), dma((ny * per, 2)), dma((ny, per, 2)), dma((ny, per, 2)),
                dma((per,)), dma((per,)),
            ],
            compiler_params=pltpu.CompilerParams(
                collective_id=0, has_side_effects=True, vmem_limit_bytes=67043328
            ),
        )(
            tokens, *weights, up_gate, up_value, down_proj, mix_gain[None], ffn_gain[None], mix_taps, mix_bias[None],
            ffn_taps, ffn_bias,
        )

    return jax.shard_map(
        on_device,
        mesh=mesh,
        in_specs=(
            P("fs", "tp"), P(), P("fs", "tp"), P("fs", "tp"), P("fs", "tp"), P(None, "tp"), P("tp"),
            P("tp", "fs"), P(), P("fs", "tp"), P("fs", "tp"), P(None, None, "tp"), P(None, "tp"),
            P("tp", "fs"),
        ),
        out_specs=P("fs", "tp"),
        check_vma=False,
    )
```

```python
import functools

import jax
import jax.numpy as jnp
from jax import lax
from jax.experimental import pallas as pl
from jax.experimental.pallas import tpu as pltpu
from jax.sharding import PartitionSpec as P

EPS = 1e-06
F32, BF16 = jnp.float32, jnp.bfloat16
MESH = pl.DeviceIdType.MESH
UP, DOWN, RIGHT, LEFT = range(4)


def grid_of(n_fs):
    nx = 1
    while nx * nx * 4 <= n_fs:
        nx *= 2
    return n_fs // nx, nx


def tiles(extent, width, body):
    whole = extent // width
    if whole:
        @pl.loop(0, whole)
        def _(i):
            body(i, pl.multiple_of(i * width, width), width)
    if extent % width:
        body(whole, whole * width, extent % width)


def causal(v, taps, bias):
    row = lax.broadcasted_iota(jnp.int32, v.shape, 0)
    first = jnp.where(row < 1, 0.0, pltpu.roll(v, 1, axis=0))
    second = jnp.where(row < 2, 0.0, pltpu.roll(v, 2, axis=0))
    return taps[2] * v + taps[1] * first + taps[0] * second + bias


def kernel(
    n_fs, n_tp, tok_in, og, ig, si, mo, ug, uv, dp,
    mix_gain, ffn_gain, mix_taps, mix_bias, ffn_taps, ffn_bias,
    out,
    w0, w1, w2, w3, f0, f1, f2,
    tok, normed, state, outer, inner, signal, gate, value,
    part1, sib1, rs1, part2, sib2, rs2, far2,
    load_sem, send_sem, recv_sem, fsend, ffar, frecv,
    tok_sib, tok_y, tok_recv, st_sib, st_y, st_z, st_recv,
    s1_send, s1_recv, p1_send, p1_recv, s2_send, s2_recv, p2_send, p2_recv, far_send, far_recv,
):
    nz, nx = grid_of(n_fs)
    fs, tp = lax.axis_index("fs"), lax.axis_index("tp")
    z, x = fs // nx, fs % nx
    ny = n_tp // 2
    y, core = tp // 2, tp % 2
    mate = tp + 1 - 2 * core
    pair = (z + 1 - 2 * (z % 2)) * nx + x
    bufs = (w0, w1, w2, w3)
    fbufs = (f0, f1, f2)
    fowns = (ug, uv, dp)
    rows, own = tok.shape[2], tok.shape[3]
    per = n_fs // n_tp
    wide = part1.shape[3]
    hidden = ug.shape[1]
    big = f0.shape[2]
    small = hidden - big
    outside = jnp.logical_or(z == 0, z == nz - 1)
    inside = jnp.logical_not(outside)

    ways = (
        (z < nz - 1, fs + nx),
        (z > 0, fs - nx),
        (x < nx - 1, fs + 1),
        (x > 0, fs - 1),
    )
    barrier = pltpu.get_barrier_semaphore()
    expected = n_tp - 1 + nz - 1 + ny - 1
    for there, peer in ways[2:]:
        expected = expected + jnp.where(there, 1, 0)

        @pl.when(there)
        def _(peer=peer):
            pl.semaphore_signal(barrier, inc=1, device_id={"fs": peer}, device_id_type=MESH)
    for r in range(1, nz):
        pl.semaphore_signal(barrier, inc=1, device_id={"fs": (z + r) % nz * nx + x}, device_id_type=MESH)
    for r in range(1, n_tp):
        pl.semaphore_signal(barrier, inc=1, device_id={"tp": (tp + r) % n_tp}, device_id_type=MESH)
    ypeers = [(y + r) % ny for r in range(1, ny)]
    for yy in ypeers:
        pl.semaphore_signal(
            barrier, inc=1, device_id={"fs": pair, "tp": yy * 2 + core}, device_id_type=MESH
        )

    loads = [pltpu.make_async_copy(a, b.at[fs], load_sem.at[i]) for i, (a, b) in enumerate(zip((og, ig, si, mo), bufs))]
    loads.append(pltpu.make_async_copy(tok_in, tok.at[0, tp], load_sem.at[4]))
    for c in loads:
        c.start()

    def span(p):
        return (0, big) if p else (big, small)

    def held(w, p, block):
        size = span(p)[1]
        return fbufs[w].at[block, pl.ds(0, size)] if w == 2 else fbufs[w].at[block, :, pl.ds(0, size)]

    def source(w, p):
        start, size = span(p)
        return fowns[w].at[pl.ds(start, size)] if w == 2 else fowns[w].at[:, pl.ds(start, size)]

    def each_part(body):
        @pl.when(outside)
        def _():
            body(0)

        @pl.when(inside)
        def _():
            body(1)

    def own_f(w, starting):
        def body(p):
            c = pltpu.make_async_copy(source(w, p), held(w, p, fs), load_sem.at[5 + w])
            if starting:
                c.start()
            else:
                c.wait()
        each_part(body)

    for w in range(3):
        own_f(w, True)
    if small < big:
        @pl.when(outside)
        def _():
            for w in range(2):
                fbufs[w][:, :, small:big] = jnp.zeros((n_fs, f0.shape[1], big - small), BF16)
            f2[:, small:big, :] = jnp.zeros((n_fs, big - small, wide), BF16)
    pl.semaphore_wait(barrier, expected)

    def cut(w):
        r = bufs[w].shape[1]
        a = max(16, (r * 13 // 16) // 16 * 16)
        return ((0, a), (a, r - a))

    def piece(w, k, block, way):
        start, size = cut(w)[k]
        ref = bufs[w].at[block, pl.ds(start, size)]
        return pltpu.make_async_remote_copy(
            src_ref=ref, dst_ref=ref,
            send_sem=send_sem.at[w, k, block, way], recv_sem=recv_sem.at[w, k, block],
            device_id={"fs": ways[way][1]}, device_id_type=MESH,
        )

    def arrive(w, k, block):
        piece(w, k, block, UP).wait_recv()

    def run(cond, c, sending):
        @pl.when(cond)
        def _():
            if sending:
                c.start()
            else:
                c.wait_send()

    def go(w, k, block, way, cond, sending):
        run(jnp.logical_and(cond, ways[way][0]), piece(w, k, block, way), sending)

    yes = z >= 0
    steps = nz
    near = jnp.minimum(z, nz - 1 - z)

    def layer(i):
        beside = z + jnp.where(i % 2 == 1, -((i + 1) // 2), i // 2)
        beyond = jnp.where(z < nz // 2, z + i - near, z - i + near)
        return jnp.where(i <= 2 * near, beside, beyond)

    def order(q):
        return ((y + 1) * (nz // ny) + q) % nz

    def spread_z(w, k, block, z0, sending):
        go(w, k, block, UP, z0 <= z, sending)
        go(w, k, block, DOWN, z0 >= z, sending)

    def along_z(w, k, z0, sending):

        @pl.when(z0 != z)
        def _():
            def relay(block):
                if sending:
                    arrive(w, k, block)
                spread_z(w, k, block, z0, sending)
            if k == 0:
                relay(z0 * nx + x)
                go(w, 0, z0 * nx + x, RIGHT, yes, sending)
                go(w, 0, z0 * nx + x, LEFT, yes, sending)
            else:
                @pl.loop(0, nx)
                def _(j):
                    relay(z0 * nx + (x + j) % nx)

    def sides(body):
        for dist in range(1, nx):
            for sign in (-1, 1):
                x0 = x + sign * dist

                @pl.when(jnp.logical_and(x0 >= 0, x0 < nx))
                def _(sign=sign, x0=x0):
                    body(x0, RIGHT if sign < 0 else LEFT)

    def along_x(w, z0, sending):
        def body(x0, way):
            if sending:
                arrive(w, 0, z0 * nx + x0)
            go(w, 0, z0 * nx + x0, way, yes, sending)
        sides(body)

    def step(w, i):
        @pl.when(i == 0)
        def _():
            row(w)

        @pl.when(jnp.logical_and(i > 0, i < steps))
        def _():
            along_z(w, 0, layer(i), True)

        @pl.when(i >= steps)
        def _():
            along_z(w, 1, layer(i - steps + 1), True)

    total_steps = 2 * steps - 1

    def pump(w, lo=0, hi=total_steps):
        @pl.loop(lo, hi)
        def _(i):
            step(w, i)

    def across(w):
        @pl.loop(0, steps)
        def _(i):
            along_x(w, layer(i), True)

    def spaced(move, lo, hi):
        def hook(j, total):
            first, last = j * (hi - lo) // total, (j + 1) * (hi - lo) // total

            @pl.loop(first, last)
            def _(i):
                move(lo + i)
        return hook

    def during(w, lo, hi):
        return spaced(lambda i: step(w, i), lo, hi)

    def begin(w, sending=True):
        if sending:
            loads[w].wait()
        for k in (1, 0):
            go(w, k, fs, RIGHT, yes, sending)
            go(w, k, fs, LEFT, yes, sending)
            spread_z(w, k, fs, z, sending)

    def row(w, sending=True):
        def body(x0, way):
            block = z * nx + x0
            if sending:
                arrive(w, 1, block)
            go(w, 1, block, way, yes, sending)
            spread_z(w, 1, block, z, sending)
        sides(body)

    def fcopy(w, p, block, src, target, sem):
        return pltpu.make_async_remote_copy(
            src_ref=src, dst_ref=held(w, p, block), send_sem=sem, recv_sem=frecv.at[w, block],
            device_id={"fs": target}, device_id_type=MESH,
        )

    def fgo(w, p, block, src, way, cond, sending):
        there, target = ways[way]
        run(jnp.logical_and(cond, there), fcopy(w, p, block, src, target, fsend.at[w, block, way]), sending)

    def farrive(w, p, block):
        fcopy(w, p, block, held(w, p, block), fs, fsend.at[w, block, 0]).wait_recv()

    up_in = jnp.logical_and(z + 1 >= 1, z + 1 <= nz - 2)
    down_in = jnp.logical_and(z - 1 >= 1, z - 1 <= nz - 2)

    def begin_fx(w, sending=True):
        for p, cond in ((0, outside), (1, inside)):
            for way in (RIGHT, LEFT):
                fgo(w, p, fs, source(w, p), way, cond, sending)

    def begin_fb(w, sending=True):
        fgo(w, 1, fs, source(w, 1), UP, up_in, sending)
        fgo(w, 1, fs, source(w, 1), DOWN, down_in, sending)

    def begin_fa(w, lo, hi, sending=True):
        stage = (z - (y + 1) * (nz // ny)) % nz + 1
        for e, end in enumerate((0, nz - 1)):
            turn = stage if w == 2 else abs(z - end)
            run(
                jnp.logical_and(z != end, jnp.logical_and(turn >= lo, turn <= hi)),
                fcopy(w, 0, fs, source(w, 0), end * nx + x, ffar.at[w, e]), sending,
            )

    outer_side = jnp.where(z < nz // 2, 0, nz - 1)

    def fz():
        @pl.when(inside)
        def _():
            block = outer_side * nx + x
            ref = held(2, 1, block)
            farrive(2, 1, block)
            fgo(2, 1, block, ref, UP, outer_side == 0, True)
            fgo(2, 1, block, ref, DOWN, outer_side != 0, True)

    def fnext(q, p):
        z0 = order(q)
        block = z0 * nx + x
        mine = z0 == z

        def both(src, cond):
            for way in (RIGHT, LEFT):
                fgo(2, p, block, src, way, cond, True)

        @pl.when(inside if p else outside)
        def _():
            both(source(2, p), mine)
            waits = jnp.logical_not(mine)
            if p:
                waits = jnp.logical_and(waits, z0 != outer_side)

            @pl.when(waits)
            def _():
                farrive(2, p, block)
            both(held(2, p, block), jnp.logical_not(mine))

    def frelay(w, i, p):
        @pl.when(inside if p else outside)
        def _():
            frelay_part(w, layer(i), p)

    def frelay_part(w, z0, p, sending=True):
        block = z0 * nx + x
        ref = held(w, p, block)

        @pl.when(z0 != z)
        def _():
            if sending:
                farrive(w, p, block)
            if p:
                fgo(w, p, block, ref, UP, jnp.logical_and(z0 < z, up_in), sending)
                fgo(w, p, block, ref, DOWN, jnp.logical_and(z0 > z, down_in), sending)
            fgo(w, p, block, ref, RIGHT, yes, sending)
            fgo(w, p, block, ref, LEFT, yes, sending)

    def fside(w, z0, sending=True):
        def part(p):
            def body(x0, way):
                block = z0 * nx + x0
                if sending:
                    farrive(w, p, block)
                fgo(w, p, block, held(w, p, block), way, yes, sending)
            sides(body)
        each_part(part)

    def fdo(*list_):
        def hook(j, total):
            for n, (w, i, p) in enumerate(list_):
                @pl.when(j == n * total // len(list_))
                def _(w=w, i=i, p=p):
                    frelay(w, i, p)
        return hook

    def fsides(w):
        @pl.loop(0, steps)
        def _(i):
            fside(w, layer(i))

    def send(ref, send, recv, to):
        return pltpu.make_async_remote_copy(
            src_ref=ref[0], dst_ref=ref[1], send_sem=send, recv_sem=recv, device_id=to, device_id_type=MESH
        )

    def got(ref, recv):
        send((ref, ref), st_z.at[0], recv, {"tp": mate}).wait_recv()

    def to_mate(buf, s, t, sib, recv):
        return send((buf.at[s, t], buf.at[s, t]), sib.at[s, t], recv.at[s, t], {"tp": mate})

    def to_ys(buf, s, ysend, recv):
        ref = buf.at[s, tp]
        return [
            send((ref, ref), ysend.at[s, r], recv.at[s, tp], {"tp": yy * 2 + core})
            for r, yy in enumerate(ypeers)
        ]

    def ag_out(buf, s, sib, ysend, recv):
        for c in to_ys(buf, s, ysend, recv):
            c.start()
        to_mate(buf, s, tp, sib, recv).start()

    def ag_relay(buf, s, sib, recv):
        for yy in ypeers:
            t = yy * 2 + core
            got(buf.at[s, t], recv.at[s, t])
            to_mate(buf, s, t, sib, recv).start()

    def ag_done(buf, s, recv):
        for yy in range(ny):
            t = yy * 2 + 1 - core
            got(buf.at[s, t], recv.at[s, t])

    def ag_sent(buf, s, sib, ysend, recv):
        for c in to_ys(buf, s, ysend, recv):
            c.wait_send()
        for yy in range(ny):
            to_mate(buf, s, yy * 2 + core, sib, recv).wait_send()

    def norm(buf, s, gain, hook):
        high = 64

        @pl.loop(0, rows // high)
        def _(m):
            at = pl.ds(pl.multiple_of(m * high, high), high)
            total = jnp.zeros((high, 1), F32)
            for t in range(n_tp):
                v = buf[s, t, at, :].astype(F32)
                total = total + jnp.sum(v * v, axis=-1, keepdims=True)
            scale = lax.rsqrt(total / (n_tp * own) + EPS)
            for t in range(n_tp):
                cols = slice(t * own, (t + 1) * own)
                v = buf[s, t, at, :].astype(F32)
                normed[s, at, cols] = (v * scale * gain[:, cols]).astype(BF16)
            hook(m, rows // high)

    mt = rows

    def none(j, total):
        pass

    def project(weights, s, dst, hook):
        n, r, c = weights.shape
        mts = rows // mt
        pieces = -(-c // 256) * mts

        def column(index, start, size):
            @pl.loop(0, mts)
            def _(m):
                at = pl.ds(pl.multiple_of(m * mt, mt), mt)
                weight = weights[:, :, pl.ds(start, size)].reshape(n * r, size)
                dst[s, at, pl.ds(start, size)] = jnp.dot(
                    normed[s, at, :], weight, preferred_element_type=F32
                ).astype(BF16)
                hook(index * mts + m, pieces)
        tiles(c, 256, column)

    def owner(block):
        t = block // per
        return t // 2, t % 2, block % per

    def out_block(weights, act, part, sib, ssend, srecv, s, block):
        @pl.loop(0, rows // mt)
        def _(m):
            at = pl.ds(pl.multiple_of(m * mt, mt), mt)
            part[block, s, at, :] = jnp.dot(
                act[s, at, :], weights[block], preferred_element_type=F32
            ).astype(BF16)
        yo, co, k = owner(block)
        run(co != core, mate_copy(part, sib, ssend, srecv, s, block), True)

    def mate_copy(part, sib, ssend, srecv, s, block):
        yo, co, k = owner(block)
        slot = yo * per + k
        return send((part.at[block, s], sib.at[slot, s]), ssend.at[slot, s], srecv.at[slot, s], {"tp": mate})

    def home_copy(part, rs, psend, precv, s, block):
        yo, co, k = owner(block)
        return send(
            (part.at[block, s], rs.at[y, k, s]), psend.at[yo, k, s], precv.at[y, k, s], {"tp": yo * 2 + core}
        )

    high = 128

    def row_tiles(body):
        @pl.loop(0, rows // high)
        def _(m):
            body(pl.ds(pl.multiple_of(m * high, high), high))

    def combine(part, sib, rs, srecv, psend, precv, s, block):
        yo, co, k = owner(block)
        slot = yo * per + k

        @pl.when(co == core)
        def _():
            got(sib.at[slot, s], srecv.at[slot, s])

            def add(at):
                part[block, s, at, :] = (
                    part[block, s, at, :].astype(F32) + sib[slot, s, at, :].astype(F32)
                ).astype(BF16)
            row_tiles(add)
            run(yo != y, home_copy(part, rs, psend, precv, s, block), True)

    def sent_home(seqs, part, sib, rs, ssend, srecv, psend, precv):
        @pl.loop(0, n_fs)
        def _(block):
            yo, co, k = owner(block)
            for s in range(seqs):
                run(co != core, mate_copy(part, sib, ssend, srecv, s, block), False)
                run(jnp.logical_and(co == core, yo != y), home_copy(part, rs, psend, precv, s, block), False)

    def collected(rs, precv):
        for k in range(per):
            for yy in ypeers:
                got(rs.at[yy, k, 0], precv.at[yy, k, 0])

    def share(part, rs, k, s, at):
        total = part[tp * per + k, s, at, :].astype(F32)
        for yy in ypeers:
            total = total + rs[yy, k, s, at, :].astype(F32)
        return total

    def add_up(base, part, rs, dst, far):
        def add(at):
            for k in range(per):
                cols = slice(k * wide, (k + 1) * wide)
                total = share(part, rs, k, 0, at)
                if far is not None:
                    total = total + far[k, at, :].astype(F32)
                dst[at, cols] = (base[at, cols].astype(F32) + total).astype(BF16)
        row_tiles(add)

    def cross_copy(k):
        return send((part2.at[tp * per + k, 1], far2.at[k]), far_send.at[k], far_recv.at[k], {"fs": pair})

    def cross():
        for k in range(per):
            for yy in ypeers:
                got(rs2.at[yy, k, 1], p2_recv.at[yy, k, 1])

            def add(at):
                part2[tp * per + k, 1, at, :] = share(part2, rs2, k, 1, at).astype(BF16)
            row_tiles(add)
            cross_copy(k).start()

    def crossed():
        for k in range(per):
            got(far2.at[k], far_recv.at[k])

    def sweep(move, form, merge):
        @pl.loop(0, nz + 2)
        def _(q):
            move(q)

            def blocks(q, body):
                @pl.loop(0, nx)
                def _(j):
                    at = jnp.where(j == 0, q, q - 1)

                    @pl.when(jnp.logical_and(at >= 0, at < nz))
                    def _():
                        body(order(at) * nx + (x + j) % nx)
            blocks(q, form)
            blocks(q - 1, merge)

    def mixer_sent():
        ag_sent(tok, 0, *tok_sems)
        sent_home(1, part1, sib1, rs1, s1_send, s1_recv, p1_send, p1_recv)
        for w in range(4):
            begin(w, False)
            row(w, False)

            @pl.loop(0, nz)
            def _(i):
                along_z(w, 0, i, False)
                along_z(w, 1, i, False)
                along_x(w, i, False)

    def ffn_sent():
        to_pair.wait_send()
        ag_sent(state, 0, *st_sems)
        ag_sent(state, 1, *st_sems)
        for w in range(3):
            begin_fx(w, False)
            begin_fb(w, False)
            begin_fa(w, 1, nz, False)

            @pl.loop(0, nz)
            def _(i):
                each_part(lambda p: frelay_part(w, i, p, False))
                fside(w, i, False)

    tok_sems = (tok_sib, tok_y, tok_recv)
    st_sems = (st_sib, st_y, st_recv)

    begin(0)
    begin(1)
    loads[4].wait()
    ag_out(tok, 0, *tok_sems)
    pump(0)
    begin(2)
    ag_relay(tok, 0, tok_sib, tok_recv)
    pump(1)
    begin(3)
    begin_fb(0)
    ag_done(tok, 0, tok_recv)
    norm(tok, 0, mix_gain, during(2, 0, 2))
    across(0)
    project(w0, 0, outer, during(2, 2, total_steps))
    across(1)
    project(w1, 0, inner, during(3, 0, steps))
    begin_fx(0)
    across(2)
    project(w2, 0, signal, during(3, steps, total_steps))
    begin_fa(0, 1, 1)
    frelay(0, 1, 1)
    frelay(0, 2, 1)

    def mixer(index, start, size):
        cols = pl.ds(start, size)
        taps = [mix_taps[j:j + 1, cols] for j in range(3)]
        v = inner[0, :, cols].astype(F32) * signal[0, :, cols].astype(F32)
        outer[0, :, cols] = (outer[0, :, cols].astype(F32) * causal(v, taps, mix_bias[:, cols])).astype(BF16)
    tiles(outer.shape[2], 128, mixer)

    def move1(q):
        @pl.when(jnp.logical_and(q >= 1, q <= nz))
        def _():
            along_x(3, order(q - 1), True)
    sweep(
        move1,
        lambda b: out_block(w3, outer, part1, sib1, s1_send, s1_recv, 0, b),
        lambda b: combine(part1, sib1, rs1, s1_recv, p1_send, p1_recv, 0, b),
    )
    begin_fb(1)
    begin_fa(0, 2, nz)
    begin_fx(1)
    frelay(0, 3, 1)
    collected(rs1, p1_recv)
    add_up(tok.at[0, tp], part1, rs1, state.at[0, tp], None)
    to_pair = send((state.at[0, tp], state.at[1, tp]), st_z.at[0], st_recv.at[1, tp], {"fs": pair})
    to_pair.start()
    ag_out(state, 0, *st_sems)
    begin_fb(2)
    frelay(1, 1, 1)
    frelay(1, 2, 1)
    frelay(0, 1, 0)
    frelay(0, 2, 0)
    frelay(0, 3, 0)
    mixer_sent()
    ag_relay(state, 0, st_sib, st_recv)
    begin_fa(1, 1, 1)
    frelay(1, 3, 1)
    got(state.at[1, tp], st_recv.at[1, tp])
    ag_out(state, 1, *st_sems)
    begin_fa(1, 2, 2)
    ag_done(state, 0, st_recv)
    norm(state, 0, ffn_gain, none)
    for w in range(3):
        own_f(w, False)
    fsides(0)
    project(f0, 0, gate, none)
    fz()
    frelay(1, 1, 0)
    begin_fa(1, 3, nz)
    frelay(1, 2, 0)
    ag_relay(state, 1, st_sib, st_recv)
    ag_done(state, 1, st_recv)
    frelay(1, 3, 0)
    begin_fa(2, 1, 2)
    for q in range(nz):
        fnext(q, 1)
    norm(state, 1, ffn_gain, none)
    project(f0, 1, gate, none)
    begin_fa(2, 3, nz)
    fsides(1)
    fnext(0, 0)
    project(f1, 0, value, none)
    fnext(1, 0)
    project(f1, 1, value, none)
    fnext(2, 0)
    shift = jnp.where(outside, big, 0)

    @pl.loop(0, jnp.where(outside, small, big) // 128)
    def _(i):
        @pl.when(i == 1)
        def _():
            fnext(3, 0)
        cols = pl.ds(pl.multiple_of(i * 128, 128), 128)
        at = pl.ds(pl.multiple_of(shift + i * 128, 128), 128)
        for s in range(2):
            g = causal(gate[s, :, cols].astype(F32), [ffn_taps[j, 0:1, at] for j in range(3)], ffn_bias[0:1, at])
            v = causal(value[s, :, cols].astype(F32), [ffn_taps[j, 1:2, at] for j in range(3)], ffn_bias[1:2, at])
            gate[s, :, cols] = (g / (1.0 + jnp.exp(-g)) * v).astype(BF16)

    def form2(s, b):
        out_block(f2, gate, part2, sib2, s2_send, s2_recv, s, b)

    def merge2(s, b):
        combine(part2, sib2, rs2, s2_recv, p2_send, p2_recv, s, b)

    @pl.loop(0, nz)
    def _(q):
        z0 = order(q)
        fside(2, z0)
        for act in (form2, merge2):
            for s in (1, 0):
                @pl.loop(0, nx)
                def _(j):
                    act(s, z0 * nx + (x + j) % nx)
    cross()
    ffn_sent()
    crossed()
    collected(rs2, p2_recv)
    add_up(state.at[0, tp], part2, rs2, out, far2)

    sent_home(2, part2, sib2, rs2, s2_send, s2_recv, p2_send, p2_recv)
    for k in range(per):
        cross_copy(k).wait_send()


def solution(mesh):
    n_fs, n_tp = mesh.shape["fs"], mesh.shape["tp"]

    def on_device(
        tokens, mix_gain, outer_gate, inner_gate, signal_in, mix_taps, mix_bias, mix_out,
        ffn_gain, up_gate, up_value, ffn_taps, ffn_bias, down_proj,
    ):
        rows, own = tokens.shape
        spare = -up_gate.shape[1] % 128
        if spare:
            up_gate, up_value, ffn_bias = (
                jnp.pad(a, ((0, 0), (0, spare))) for a in (up_gate, up_value, ffn_bias)
            )
            ffn_taps = jnp.pad(ffn_taps, ((0, 0), (0, 0), (0, spare)))
            down_proj = jnp.pad(down_proj, ((0, spare), (0, 0)))
        weights = (outer_gate, inner_gate, signal_in, mix_out)
        chan, hidden = outer_gate.shape[1], up_gate.shape[1]
        depth, wide = outer_gate.shape[0], mix_out.shape[1]
        big = hidden - hidden // 256 * 128
        model = own * n_tp
        hbm = pl.BlockSpec(memory_space=pl.ANY)
        vmem = pl.BlockSpec(memory_space=pltpu.VMEM)
        dma = pltpu.SemaphoreType.DMA
        per, ny = n_fs // n_tp, n_tp // 2
        return pl.pallas_call(
            functools.partial(kernel, n_fs, n_tp),
            out_shape=jax.ShapeDtypeStruct(tokens.shape, BF16),
            in_specs=[hbm] * 8 + [vmem] * 6,
            out_specs=vmem,
            scratch_shapes=[pltpu.VMEM((n_fs, *w.shape), BF16) for w in weights]
            + [
                pltpu.VMEM((n_fs, depth, big), BF16),
                pltpu.VMEM((n_fs, depth, big), BF16),
                pltpu.VMEM((n_fs, big, wide), BF16),
                pltpu.VMEM((1, n_tp, rows, own), BF16),
                pltpu.VMEM((2, rows, model), BF16),
                pltpu.VMEM((2, n_tp, rows, own), BF16),
                pltpu.VMEM((1, rows, chan), BF16),
                pltpu.VMEM((1, rows, chan), BF16),
                pltpu.VMEM((1, rows, chan), BF16),
                pltpu.VMEM((2, rows, big), BF16),
                pltpu.VMEM((2, rows, big), BF16),
                pltpu.VMEM((n_fs, 1, rows, wide), BF16),
                pltpu.VMEM((ny * per, 1, rows, wide), BF16),
                pltpu.VMEM((ny, per, 1, rows, wide), BF16),
                pltpu.VMEM((n_fs, 2, rows, wide), BF16),
                pltpu.VMEM((ny * per, 2, rows, wide), BF16),
                pltpu.VMEM((ny, per, 2, rows, wide), BF16),
                pltpu.VMEM((per, rows, wide), BF16),
                dma((8,)),
                dma((4, 2, n_fs, 4)),
                dma((4, 2, n_fs)),
                dma((3, n_fs, 4)),
                dma((3, 2)),
                dma((3, n_fs)),
                dma((1, n_tp)), dma((1, ny)), dma((1, n_tp)),
                dma((2, n_tp)), dma((2, ny)), dma((1,)), dma((2, n_tp)),
                dma((ny * per, 1)), dma((ny * per, 1)), dma((ny, per, 1)), dma((ny, per, 1)),
                dma((ny * per, 2)), dma((ny * per, 2)), dma((ny, per, 2)), dma((ny, per, 2)),
                dma((per,)), dma((per,)),
            ],
            compiler_params=pltpu.CompilerParams(
                collective_id=0, has_side_effects=True, vmem_limit_bytes=67043328
            ),
        )(
            tokens, *weights, up_gate, up_value, down_proj, mix_gain[None], ffn_gain[None], mix_taps, mix_bias[None],
            jnp.transpose(ffn_taps, (1, 0, 2)), ffn_bias,
        )

    return jax.shard_map(
        on_device,
        mesh=mesh,
        in_specs=(
            P("fs", "tp"), P(), P("fs", "tp"), P("fs", "tp"), P("fs", "tp"), P(None, "tp"), P("tp"),
            P("tp", "fs"), P(), P("fs", "tp"), P("fs", "tp"), P(None, None, "tp"), P(None, "tp"),
            P("tp", "fs"),
        ),
        out_specs=P("fs", "tp"),
        check_vma=False,
    )
```

```python
import functools

import jax
import jax.numpy as jnp
from jax import lax
from jax.experimental import pallas as pl
from jax.experimental.pallas import tpu as pltpu
from jax.sharding import PartitionSpec as P

EPS = 1e-06
F32, BF16 = jnp.float32, jnp.bfloat16
MESH = pl.DeviceIdType.MESH
UP, DOWN, RIGHT, LEFT = range(4)


def grid_of(n_fs):
    nx = 1
    while nx * nx * 4 <= n_fs:
        nx *= 2
    return n_fs // nx, nx


def tiles(extent, width, body):
    whole = extent // width
    if whole:
        @pl.loop(0, whole)
        def _(i):
            body(i, pl.multiple_of(i * width, width), width)
    if extent % width:
        body(whole, whole * width, extent % width)


def causal(v, taps, bias):
    row = lax.broadcasted_iota(jnp.int32, v.shape, 0)
    first = jnp.where(row < 1, 0.0, pltpu.roll(v, 1, axis=0))
    second = jnp.where(row < 2, 0.0, pltpu.roll(v, 2, axis=0))
    return taps[2] * v + taps[1] * first + taps[0] * second + bias


def kernel(
    n_fs, n_tp, tok_in, og, ig, si, mo, ug, uv, dp,
    mix_gain, ffn_gain, mix_taps, mix_bias, ffn_taps, ffn_bias,
    out,
    w0, w1, w2, w3, f0, f1, f2,
    tok, normed, state, outer, inner, signal, gate, value,
    part1, sib1, rs1, part2, sib2, rs2, far2,
    load_sem, send_sem, row_sem, recv_sem, fsend, ffar, frecv,
    tok_sib, tok_y, tok_recv, st_sib, st_y, st_z, st_recv,
    s1_send, s1_recv, p1_send, p1_recv, s2_send, s2_recv, p2_send, p2_recv, far_send, far_recv,
):
    nz, nx = grid_of(n_fs)
    fs, tp = lax.axis_index("fs"), lax.axis_index("tp")
    z, x = fs // nx, fs % nx
    ny = n_tp // 2
    y, core = tp // 2, tp % 2
    mate = tp + 1 - 2 * core
    pair = (z + 1 - 2 * (z % 2)) * nx + x
    bufs = (w0, w1, w2, w3)
    fbufs = (f0, f1, f2)
    fowns = (ug, uv, dp)
    rows, own = tok.shape[2], tok.shape[3]
    per = n_fs // n_tp
    wide = part1.shape[3]
    hidden = ug.shape[1]
    big = f0.shape[2]
    small = hidden - big
    outside = jnp.logical_or(z == 0, z == nz - 1)
    inside = jnp.logical_not(outside)

    ways = (
        (z < nz - 1, fs + nx),
        (z > 0, fs - nx),
        (x < nx - 1, fs + 1),
        (x > 0, fs - 1),
    )
    barrier = pltpu.get_barrier_semaphore()
    expected = n_tp - 1 + nz - 1 + ny - 1
    for there, peer in ways[2:]:
        expected = expected + jnp.where(there, 1, 0)

        @pl.when(there)
        def _(peer=peer):
            pl.semaphore_signal(barrier, inc=1, device_id={"fs": peer}, device_id_type=MESH)
    for r in range(1, nz):
        pl.semaphore_signal(barrier, inc=1, device_id={"fs": (z + r) % nz * nx + x}, device_id_type=MESH)
    for r in range(1, n_tp):
        pl.semaphore_signal(barrier, inc=1, device_id={"tp": (tp + r) % n_tp}, device_id_type=MESH)
    ypeers = [(y + r) % ny for r in range(1, ny)]
    for yy in ypeers:
        pl.semaphore_signal(
            barrier, inc=1, device_id={"fs": pair, "tp": yy * 2 + core}, device_id_type=MESH
        )

    loads = [pltpu.make_async_copy(a, b.at[fs], load_sem.at[i]) for i, (a, b) in enumerate(zip((og, ig, si, mo), bufs))]
    loads.append(pltpu.make_async_copy(tok_in, tok.at[0, tp], load_sem.at[4]))
    for c in loads:
        c.start()

    def span(p):
        return (0, big) if p else (big, small)

    def held(w, p, block):
        size = span(p)[1]
        return fbufs[w].at[block, pl.ds(0, size)] if w == 2 else fbufs[w].at[block, :, pl.ds(0, size)]

    def source(w, p):
        start, size = span(p)
        return fowns[w].at[pl.ds(start, size)] if w == 2 else fowns[w].at[:, pl.ds(start, size)]

    def each_part(body):
        @pl.when(outside)
        def _():
            body(0)

        @pl.when(inside)
        def _():
            body(1)

    def own_f(w, starting):
        def body(p):
            c = pltpu.make_async_copy(source(w, p), held(w, p, fs), load_sem.at[5 + w])
            if starting:
                c.start()
            else:
                c.wait()
        each_part(body)

    for w in range(3):
        own_f(w, True)
    pl.semaphore_wait(barrier, expected)

    def cut(w):
        r = bufs[w].shape[1]
        a = max(16, (r * 13 // 16) // 16 * 16)
        return ((0, a), (a, r - a))

    def slot(block, way, wide_row):
        z0, x0 = block // nx, block % nx
        if wide_row:
            return jnp.where(z0 == z, x0 * 4 + way, nx * 4 + block)
        return jnp.where(x0 == x, z0 * 4 + way, nz * 4 + block)

    def piece(w, k, block, way):
        start, size = cut(w)[k]
        ref = bufs[w].at[block, pl.ds(start, size)]
        return pltpu.make_async_remote_copy(
            src_ref=ref, dst_ref=ref,
            send_sem=(row_sem if k else send_sem).at[w, slot(block, way, k)], recv_sem=recv_sem.at[w, k, block],
            device_id={"fs": ways[way][1]}, device_id_type=MESH,
        )

    def arrive(w, k, block):
        piece(w, k, block, UP).wait_recv()

    def run(cond, c, sending):
        @pl.when(cond)
        def _():
            if sending:
                c.start()
            else:
                c.wait_send()

    def go(w, k, block, way, cond, sending):
        run(jnp.logical_and(cond, ways[way][0]), piece(w, k, block, way), sending)

    yes = z >= 0
    steps = nz
    near = jnp.minimum(z, nz - 1 - z)

    def layer(i):
        beside = z + jnp.where(i % 2 == 1, -((i + 1) // 2), i // 2)
        beyond = jnp.where(z < nz // 2, z + i - near, z - i + near)
        return jnp.where(i <= 2 * near, beside, beyond)

    def order(q):
        return ((y + 1) * (nz // ny) + q) % nz

    def spread_z(w, k, block, z0, sending):
        go(w, k, block, UP, z0 <= z, sending)
        go(w, k, block, DOWN, z0 >= z, sending)

    def along_z(w, k, z0, sending):

        @pl.when(z0 != z)
        def _():
            def relay(block):
                if sending:
                    arrive(w, k, block)
                spread_z(w, k, block, z0, sending)
            if k == 0:
                relay(z0 * nx + x)
                go(w, 0, z0 * nx + x, RIGHT, yes, sending)
                go(w, 0, z0 * nx + x, LEFT, yes, sending)
            else:
                @pl.loop(0, nx)
                def _(j):
                    relay(z0 * nx + (x + j) % nx)

    def sides(body):
        for dist in range(1, nx):
            for sign in (-1, 1):
                x0 = x + sign * dist

                @pl.when(jnp.logical_and(x0 >= 0, x0 < nx))
                def _(sign=sign, x0=x0):
                    body(x0, RIGHT if sign < 0 else LEFT)

    def along_x(w, z0, sending):
        def body(x0, way):
            if sending:
                arrive(w, 0, z0 * nx + x0)
            go(w, 0, z0 * nx + x0, way, yes, sending)
        sides(body)

    def step(w, i):
        @pl.when(i == 0)
        def _():
            row(w)

        @pl.when(jnp.logical_and(i > 0, i < steps))
        def _():
            along_z(w, 0, layer(i), True)

        @pl.when(i >= steps)
        def _():
            along_z(w, 1, layer(i - steps + 1), True)

    total_steps = 2 * steps - 1

    def pump(w, lo=0, hi=total_steps):
        @pl.loop(lo, hi)
        def _(i):
            step(w, i)

    def across(w):
        @pl.loop(0, steps)
        def _(i):
            along_x(w, layer(i), True)

    def spaced(move, lo, hi):
        def hook(j, total):
            first, last = j * (hi - lo) // total, (j + 1) * (hi - lo) // total

            @pl.loop(first, last)
            def _(i):
                move(lo + i)
        return hook

    def during(w, lo, hi):
        return spaced(lambda i: step(w, i), lo, hi)

    def begin(w, sending=True):
        if sending:
            loads[w].wait()
        for k in (1, 0):
            go(w, k, fs, RIGHT, yes, sending)
            go(w, k, fs, LEFT, yes, sending)
            spread_z(w, k, fs, z, sending)

    def row(w, sending=True):
        def body(x0, way):
            block = z * nx + x0
            if sending:
                arrive(w, 1, block)
            go(w, 1, block, way, yes, sending)
            spread_z(w, 1, block, z, sending)
        sides(body)

    def fcopy(w, p, block, src, target, sem):
        return pltpu.make_async_remote_copy(
            src_ref=src, dst_ref=held(w, p, block), send_sem=sem, recv_sem=frecv.at[w, block],
            device_id={"fs": target}, device_id_type=MESH,
        )

    def fgo(w, p, block, src, way, cond, sending):
        there, target = ways[way]
        run(jnp.logical_and(cond, there), fcopy(w, p, block, src, target, fsend.at[w, slot(block, way, 0)]), sending)

    def farrive(w, p, block):
        fcopy(w, p, block, held(w, p, block), fs, fsend.at[w, 0]).wait_recv()

    up_in = jnp.logical_and(z + 1 >= 1, z + 1 <= nz - 2)
    down_in = jnp.logical_and(z - 1 >= 1, z - 1 <= nz - 2)

    def begin_fx(w, sending=True):
        for p, cond in ((0, outside), (1, inside)):
            for way in (RIGHT, LEFT):
                fgo(w, p, fs, source(w, p), way, cond, sending)

    def begin_fb(w, sending=True):
        fgo(w, 1, fs, source(w, 1), UP, up_in, sending)
        fgo(w, 1, fs, source(w, 1), DOWN, down_in, sending)

    def begin_fa(w, lo, hi, sending=True):
        stage = (z - (y + 1) * (nz // ny)) % nz + 1
        for e, end in enumerate((0, nz - 1)):
            turn = stage if w == 2 else abs(z - end)
            run(
                jnp.logical_and(z != end, jnp.logical_and(turn >= lo, turn <= hi)),
                fcopy(w, 0, fs, source(w, 0), end * nx + x, ffar.at[w, e]), sending,
            )

    outer_side = jnp.where(z < nz // 2, 0, nz - 1)

    def fz():
        @pl.when(inside)
        def _():
            block = outer_side * nx + x
            ref = held(2, 1, block)
            farrive(2, 1, block)
            fgo(2, 1, block, ref, UP, outer_side == 0, True)
            fgo(2, 1, block, ref, DOWN, outer_side != 0, True)

    def fnext(q, p):
        z0 = order(q)
        block = z0 * nx + x
        mine = z0 == z

        def both(src, cond):
            for way in (RIGHT, LEFT):
                fgo(2, p, block, src, way, cond, True)

        @pl.when(inside if p else outside)
        def _():
            if p:
                both(source(2, p), mine)
            waits = jnp.logical_not(mine)
            if p:
                waits = jnp.logical_and(waits, z0 != outer_side)

            @pl.when(waits)
            def _():
                farrive(2, p, block)
            both(held(2, p, block), jnp.logical_not(mine))

    def frelay(w, i, p):
        @pl.when(inside if p else outside)
        def _():
            frelay_part(w, layer(i), p)

    def frelay_part(w, z0, p, sending=True):
        block = z0 * nx + x
        ref = held(w, p, block)

        @pl.when(z0 != z)
        def _():
            if sending:
                farrive(w, p, block)
            if p:
                fgo(w, p, block, ref, UP, jnp.logical_and(z0 < z, up_in), sending)
                fgo(w, p, block, ref, DOWN, jnp.logical_and(z0 > z, down_in), sending)
            fgo(w, p, block, ref, RIGHT, yes, sending)
            fgo(w, p, block, ref, LEFT, yes, sending)

    def fside(w, z0, sending=True):
        def part(p):
            def body(x0, way):
                block = z0 * nx + x0
                if sending:
                    farrive(w, p, block)
                fgo(w, p, block, held(w, p, block), way, yes, sending)
            sides(body)
        each_part(part)

    def fdo(*list_):
        def hook(j, total):
            for n, (w, i, p) in enumerate(list_):
                @pl.when(j == n * total // len(list_))
                def _(w=w, i=i, p=p):
                    frelay(w, i, p)
        return hook

    def fsides(w):
        @pl.loop(0, steps)
        def _(i):
            fside(w, layer(i))

    def send(ref, send, recv, to):
        return pltpu.make_async_remote_copy(
            src_ref=ref[0], dst_ref=ref[1], send_sem=send, recv_sem=recv, device_id=to, device_id_type=MESH
        )

    def got(ref, recv):
        send((ref, ref), st_z.at[0], recv, {"tp": mate}).wait_recv()

    def to_mate(buf, s, t, sib, recv):
        return send((buf.at[s, t], buf.at[s, t]), sib.at[s, t], recv.at[s, t], {"tp": mate})

    def to_ys(buf, s, ysend, recv):
        ref = buf.at[s, tp]
        return [
            send((ref, ref), ysend.at[s, r], recv.at[s, tp], {"tp": yy * 2 + core})
            for r, yy in enumerate(ypeers)
        ]

    def ag_out(buf, s, sib, ysend, recv):
        for c in to_ys(buf, s, ysend, recv):
            c.start()
        to_mate(buf, s, tp, sib, recv).start()

    def ag_relay(buf, s, sib, recv):
        for yy in ypeers:
            t = yy * 2 + core
            got(buf.at[s, t], recv.at[s, t])
            to_mate(buf, s, t, sib, recv).start()

    def ag_done(buf, s, recv):
        for yy in range(ny):
            t = yy * 2 + 1 - core
            got(buf.at[s, t], recv.at[s, t])

    def ag_sent(buf, s, sib, ysend, recv):
        for c in to_ys(buf, s, ysend, recv):
            c.wait_send()
        for yy in range(ny):
            to_mate(buf, s, yy * 2 + core, sib, recv).wait_send()

    def norm(buf, s, gain, hook):
        high = 64

        @pl.loop(0, rows // high)
        def _(m):
            at = pl.ds(pl.multiple_of(m * high, high), high)
            total = jnp.zeros((high, 1), F32)
            for t in range(n_tp):
                v = buf[s, t, at, :].astype(F32)
                total = total + jnp.sum(v * v, axis=-1, keepdims=True)
            scale = lax.rsqrt(total / (n_tp * own) + EPS)
            for t in range(n_tp):
                cols = slice(t * own, (t + 1) * own)
                v = buf[s, t, at, :].astype(F32)
                normed[s, at, cols] = (v * scale * gain[:, cols]).astype(BF16)
            hook(m, rows // high)

    mt = rows

    def none(j, total):
        pass

    def project(weights, s, dst, hook):
        n, r, c = weights.shape
        mts = rows // mt
        pieces = -(-c // 256) * mts

        def column(index, start, size):
            @pl.loop(0, mts)
            def _(m):
                at = pl.ds(pl.multiple_of(m * mt, mt), mt)
                weight = weights[:, :, pl.ds(start, size)].reshape(n * r, size)
                dst[s, at, pl.ds(start, size)] = jnp.dot(
                    normed[s, at, :], weight, preferred_element_type=F32
                ).astype(BF16)
                hook(index * mts + m, pieces)
        tiles(c, 256, column)

    def owner(block):
        t = block // per
        return t // 2, t % 2, block % per

    def out_block(weights, act, part, sib, ssend, srecv, s, block):
        @pl.loop(0, rows // mt)
        def _(m):
            at = pl.ds(pl.multiple_of(m * mt, mt), mt)
            part[block, s, at, :] = jnp.dot(
                act[s, at, :], weights[block], preferred_element_type=F32
            ).astype(BF16)
        yo, co, k = owner(block)
        run(co != core, mate_copy(part, sib, ssend, srecv, s, block), True)

    def mate_copy(part, sib, ssend, srecv, s, block):
        yo, co, k = owner(block)
        slot = yo * per + k
        return send((part.at[block, s], sib.at[slot, s]), ssend.at[slot, s], srecv.at[slot, s], {"tp": mate})

    def home_copy(part, rs, psend, precv, s, block):
        yo, co, k = owner(block)
        return send(
            (part.at[block, s], rs.at[y, k, s]), psend.at[yo, k, s], precv.at[y, k, s], {"tp": yo * 2 + core}
        )

    high = 128

    def row_tiles(body):
        @pl.loop(0, rows // high)
        def _(m):
            body(pl.ds(pl.multiple_of(m * high, high), high))

    def combine(part, sib, rs, srecv, psend, precv, s, block):
        yo, co, k = owner(block)
        slot = yo * per + k

        @pl.when(co == core)
        def _():
            got(sib.at[slot, s], srecv.at[slot, s])

            def add(at):
                part[block, s, at, :] = (
                    part[block, s, at, :].astype(F32) + sib[slot, s, at, :].astype(F32)
                ).astype(BF16)
            row_tiles(add)
            run(yo != y, home_copy(part, rs, psend, precv, s, block), True)

    def sent_home(seqs, part, sib, rs, ssend, srecv, psend, precv):
        @pl.loop(0, n_fs)
        def _(block):
            yo, co, k = owner(block)
            for s in range(seqs):
                run(co != core, mate_copy(part, sib, ssend, srecv, s, block), False)
                run(jnp.logical_and(co == core, yo != y), home_copy(part, rs, psend, precv, s, block), False)

    def collected(rs, precv):
        for k in range(per):
            for yy in ypeers:
                got(rs.at[yy, k, 0], precv.at[yy, k, 0])

    def share(part, rs, k, s, at):
        total = part[tp * per + k, s, at, :].astype(F32)
        for yy in ypeers:
            total = total + rs[yy, k, s, at, :].astype(F32)
        return total

    def add_up(base, part, rs, dst, far):
        def add(at):
            for k in range(per):
                cols = slice(k * wide, (k + 1) * wide)
                total = share(part, rs, k, 0, at)
                if far is not None:
                    total = total + far[k, at, :].astype(F32)
                dst[at, cols] = (base[at, cols].astype(F32) + total).astype(BF16)
        row_tiles(add)

    def cross_copy(k):
        return send((part2.at[tp * per + k, 1], far2.at[k]), far_send.at[k], far_recv.at[k], {"fs": pair})

    def cross():
        for k in range(per):
            for yy in ypeers:
                got(rs2.at[yy, k, 1], p2_recv.at[yy, k, 1])

            def add(at):
                part2[tp * per + k, 1, at, :] = share(part2, rs2, k, 1, at).astype(BF16)
            row_tiles(add)
            cross_copy(k).start()

    def crossed():
        for k in range(per):
            got(far2.at[k], far_recv.at[k])

    def sweep(move, form, merge):
        @pl.loop(0, nz + 2)
        def _(q):
            move(q)

            def blocks(q, body):
                @pl.loop(0, nx)
                def _(j):
                    at = jnp.where(j == 0, q, q - 1)

                    @pl.when(jnp.logical_and(at >= 0, at < nz))
                    def _():
                        body(order(at) * nx + (x + j) % nx)
            blocks(q, form)
            blocks(q - 1, merge)

    def mixer_sent():
        ag_sent(tok, 0, *tok_sems)
        sent_home(1, part1, sib1, rs1, s1_send, s1_recv, p1_send, p1_recv)
        for w in range(4):
            begin(w, False)
            row(w, False)

            @pl.loop(0, nz)
            def _(i):
                along_z(w, 0, i, False)
                along_z(w, 1, i, False)
                along_x(w, i, False)

    def ffn_sent():
        to_pair.wait_send()
        ag_sent(state, 0, *st_sems)
        ag_sent(state, 1, *st_sems)
        for w in range(3):
            begin_fx(w, False)
            begin_fb(w, False)
            begin_fa(w, 1, nz, False)

            @pl.loop(0, nz)
            def _(i):
                each_part(lambda p: frelay_part(w, i, p, False))
                fside(w, i, False)

    tok_sems = (tok_sib, tok_y, tok_recv)
    st_sems = (st_sib, st_y, st_recv)

    begin(0)
    begin(1)
    loads[4].wait()
    ag_out(tok, 0, *tok_sems)
    if small < big:
        @pl.when(outside)
        def _():
            for w in range(2):
                fbufs[w][:, :, small:big] = jnp.zeros((n_fs, f0.shape[1], big - small), BF16)
            f2[:, small:big, :] = jnp.zeros((n_fs, big - small, wide), BF16)
    pump(0)
    begin(2)
    ag_relay(tok, 0, tok_sib, tok_recv)
    pump(1)
    begin(3)
    begin_fb(0)
    ag_done(tok, 0, tok_recv)
    norm(tok, 0, mix_gain, during(2, 0, 2))
    across(0)
    project(w0, 0, outer, during(2, 2, total_steps))
    across(1)
    project(w1, 0, inner, during(3, 0, steps))
    begin_fx(0)
    across(2)
    project(w2, 0, signal, during(3, steps, total_steps))
    begin_fa(0, 1, 1)
    frelay(0, 1, 1)
    frelay(0, 2, 1)

    def mixer(index, start, size):
        cols = pl.ds(start, size)
        taps = [mix_taps[j:j + 1, cols] for j in range(3)]
        v = inner[0, :, cols].astype(F32) * signal[0, :, cols].astype(F32)
        outer[0, :, cols] = (outer[0, :, cols].astype(F32) * causal(v, taps, mix_bias[:, cols])).astype(BF16)
    tiles(outer.shape[2], 128, mixer)

    def move1(q):
        @pl.when(jnp.logical_and(q >= 1, q <= nz))
        def _():
            along_x(3, order(q - 1), True)
    sweep(
        move1,
        lambda b: out_block(w3, outer, part1, sib1, s1_send, s1_recv, 0, b),
        lambda b: combine(part1, sib1, rs1, s1_recv, p1_send, p1_recv, 0, b),
    )
    begin_fb(1)
    begin_fa(0, 2, nz)
    begin_fx(1)
    frelay(0, 3, 1)
    collected(rs1, p1_recv)
    add_up(tok.at[0, tp], part1, rs1, state.at[0, tp], None)
    to_pair = send((state.at[0, tp], state.at[1, tp]), st_z.at[0], st_recv.at[1, tp], {"fs": pair})
    to_pair.start()
    ag_out(state, 0, *st_sems)
    begin_fb(2)
    frelay(1, 1, 1)
    frelay(1, 2, 1)
    frelay(0, 1, 0)
    frelay(0, 2, 0)
    frelay(0, 3, 0)
    for way in (RIGHT, LEFT):
        fgo(2, 0, fs, source(2, 0), way, outside, True)
    mixer_sent()
    ag_relay(state, 0, st_sib, st_recv)
    begin_fa(1, 1, 1)
    frelay(1, 3, 1)
    got(state.at[1, tp], st_recv.at[1, tp])
    ag_out(state, 1, *st_sems)
    begin_fa(1, 2, 2)
    ag_done(state, 0, st_recv)
    norm(state, 0, ffn_gain, none)
    for w in range(3):
        own_f(w, False)
    fsides(0)
    project(f0, 0, gate, none)
    fz()
    frelay(1, 1, 0)
    begin_fa(1, 3, nz)
    frelay(1, 2, 0)
    ag_relay(state, 1, st_sib, st_recv)
    ag_done(state, 1, st_recv)
    frelay(1, 3, 0)
    begin_fa(2, 1, 2)
    for q in range(nz):
        fnext(q, 1)
    norm(state, 1, ffn_gain, none)
    project(f0, 1, gate, none)
    begin_fa(2, 3, nz)
    fsides(1)
    fnext(0, 0)
    project(f1, 0, value, none)
    fnext(1, 0)
    project(f1, 1, value, none)
    fnext(2, 0)
    shift = jnp.where(outside, big, 0)

    @pl.loop(0, jnp.where(outside, small, big) // 128)
    def _(i):
        @pl.when(i == 1)
        def _():
            fnext(3, 0)
        cols = pl.ds(pl.multiple_of(i * 128, 128), 128)
        at = pl.ds(pl.multiple_of(shift + i * 128, 128), 128)
        for s in range(2):
            g = causal(gate[s, :, cols].astype(F32), [ffn_taps[j, 0:1, at] for j in range(3)], ffn_bias[0:1, at])
            v = causal(value[s, :, cols].astype(F32), [ffn_taps[j, 1:2, at] for j in range(3)], ffn_bias[1:2, at])
            gate[s, :, cols] = (g / (1.0 + jnp.exp(-g)) * v).astype(BF16)

    def form2(s, b):
        out_block(f2, gate, part2, sib2, s2_send, s2_recv, s, b)

    def merge2(s, b):
        combine(part2, sib2, rs2, s2_recv, p2_send, p2_recv, s, b)

    @pl.loop(0, nz)
    def _(q):
        z0 = order(q)
        fside(2, z0)
        for act in (form2, merge2):
            for s in (1, 0):
                @pl.loop(0, nx)
                def _(j):
                    act(s, z0 * nx + (x + j) % nx)
    cross()
    ffn_sent()
    crossed()
    collected(rs2, p2_recv)
    add_up(state.at[0, tp], part2, rs2, out, far2)

    sent_home(2, part2, sib2, rs2, s2_send, s2_recv, p2_send, p2_recv)
    for k in range(per):
        cross_copy(k).wait_send()


def solution(mesh):
    n_fs, n_tp = mesh.shape["fs"], mesh.shape["tp"]

    def on_device(
        tokens, mix_gain, outer_gate, inner_gate, signal_in, mix_taps, mix_bias, mix_out,
        ffn_gain, up_gate, up_value, ffn_taps, ffn_bias, down_proj,
    ):
        rows, own = tokens.shape
        spare = -up_gate.shape[1] % 128
        if spare:
            up_gate, up_value, ffn_bias = (
                jnp.pad(a, ((0, 0), (0, spare))) for a in (up_gate, up_value, ffn_bias)
            )
            ffn_taps = jnp.pad(ffn_taps, ((0, 0), (0, 0), (0, spare)))
            down_proj = jnp.pad(down_proj, ((0, spare), (0, 0)))
        weights = (outer_gate, inner_gate, signal_in, mix_out)
        chan, hidden = outer_gate.shape[1], up_gate.shape[1]
        depth, wide = outer_gate.shape[0], mix_out.shape[1]
        big = hidden - hidden // 256 * 128
        model = own * n_tp
        hbm = pl.BlockSpec(memory_space=pl.ANY)
        vmem = pl.BlockSpec(memory_space=pltpu.VMEM)
        dma = pltpu.SemaphoreType.DMA
        per, ny = n_fs // n_tp, n_tp // 2
        nz, nx = grid_of(n_fs)
        return pl.pallas_call(
            functools.partial(kernel, n_fs, n_tp),
            out_shape=pltpu.VMEM(tokens.shape, BF16),
            in_specs=[hbm] * 8 + [vmem] * 6,
            out_specs=vmem,
            scratch_shapes=[pltpu.VMEM((n_fs, *w.shape), BF16) for w in weights]
            + [
                pltpu.VMEM((n_fs, depth, big), BF16),
                pltpu.VMEM((n_fs, depth, big), BF16),
                pltpu.VMEM((n_fs, big, wide), BF16),
                pltpu.VMEM((1, n_tp, rows, own), BF16),
                pltpu.VMEM((2, rows, model), BF16),
                pltpu.VMEM((2, n_tp, rows, own), BF16),
                pltpu.VMEM((1, rows, chan), BF16),
                pltpu.VMEM((1, rows, chan), BF16),
                pltpu.VMEM((1, rows, chan), BF16),
                pltpu.VMEM((2, rows, big), BF16),
                pltpu.VMEM((2, rows, big), BF16),
                pltpu.VMEM((n_fs, 1, rows, wide), BF16),
                pltpu.VMEM((ny * per, 1, rows, wide), BF16),
                pltpu.VMEM((ny, per, 1, rows, wide), BF16),
                pltpu.VMEM((n_fs, 2, rows, wide), BF16),
                pltpu.VMEM((ny * per, 2, rows, wide), BF16),
                pltpu.VMEM((ny, per, 2, rows, wide), BF16),
                pltpu.VMEM((per, rows, wide), BF16),
                dma((8,)),
                dma((4, 4 * nz + n_fs)),
                dma((4, 4 * nx + n_fs)),
                dma((4, 2, n_fs)),
                dma((3, 4 * nz + n_fs)),
                dma((3, 2)),
                dma((3, n_fs)),
                dma((1, n_tp)), dma((1, ny)), dma((1, n_tp)),
                dma((2, n_tp)), dma((2, ny)), dma((1,)), dma((2, n_tp)),
                dma((ny * per, 1)), dma((ny * per, 1)), dma((ny, per, 1)), dma((ny, per, 1)),
                dma((ny * per, 2)), dma((ny * per, 2)), dma((ny, per, 2)), dma((ny, per, 2)),
                dma((per,)), dma((per,)),
            ],
            compiler_params=pltpu.CompilerParams(
                collective_id=0, has_side_effects=True, vmem_limit_bytes=65 * 2**20 - 2**20 * 2
            ),
        )(
            tokens, *weights, up_gate, up_value, down_proj, mix_gain[None], ffn_gain[None], mix_taps, mix_bias[None],
            jnp.transpose(ffn_taps, (1, 0, 2)), ffn_bias,
        )

    return jax.shard_map(
        on_device,
        mesh=mesh,
        in_specs=(
            P("fs", "tp"), P(), P("fs", "tp"), P("fs", "tp"), P("fs", "tp"), P(None, "tp"), P("tp"),
            P("tp", "fs"), P(), P("fs", "tp"), P("fs", "tp"), P(None, None, "tp"), P(None, "tp"),
            P("tp", "fs"),
        ),
        out_specs=P("fs", "tp"),
        check_vma=False,
    )
```
